32 devices in a mesh: sp: 4 (over z), tp: 4 (over y, x), dp: 2 (over core).
Axes of the slice: x: 2, y: 2, z: 4, core: 2. Of those that a mesh axis runs over, the one named last changes fastest.
Arguments:
- latent: bfloat16 [2, 1024, 2048], P('dp', ('sp', 'tp')), may hold values from -6 to 6
- condition: bfloat16 [2, 2048], P('dp', ('sp', 'tp')), may hold values from -6 to 6
- context: bfloat16 [2, 32, 2048], P('dp', 'sp'), may hold values from -6 to 6
- context_vector: bfloat16 [2048], P(('sp', 'tp')), may hold values from -6 to 6
- modulator: bfloat16 [2048, 6144], P(('sp', 'tp')), may hold values from -0.3125 to 0.3125
- norm_gain: float32 [2048], replicated, may hold values from 0.1 to 1.9
- query_weight: bfloat16 [2048, 512], P(None, 'tp'), may hold values from -4 to 4
- key_weight: bfloat16 [2048, 512], P(None, 'tp'), may hold values from -0.125 to 0.125
- value_weight: bfloat16 [2048, 512], P(None, 'tp'), may hold values from -0.125 to 0.125
- head_gain: float32 [128], replicated, may hold values from 0.1 to 1.9
- lambdas: float32 [4], P('tp'), may hold values from 0.3 to 0.8
- context_bias: float32 [4, 2], P('tp'), may hold values from 1.3 to 2.7
- out_weight: bfloat16 [512, 2048], P('tp'), may hold values from -0.25 to 0.25
Outputs:
- updated: bfloat16 [2, 1024, 2048], P('dp', ('sp', 'tp'))
The draws below stay inside these ranges and needn't reach their ends.
All inputs are finite; a program needn't handle non-finite values.
Results may differ from the reference program's by a relative error of at most 0.024.
Values may be sent and summed in bfloat16 or wider, within the bound.
A program may use at most 64 MiB of HBM per device.

```python
import math
import jax
import jax.numpy as jnp
from jax import lax

D = 2048
HEADS = 4
HEAD = 64
SEQ = 1024
CTX = 32
SAMPLES = 2


def query_key_pair(key):
    key_spread = (1.5 * D) ** (-0.5)
    query_spread = (3.0 * D) ** (-0.5)
    key_part = key_spread * jax.random.normal(jax.random.fold_in(key, 11), (D, HEADS, 2, HEAD), jnp.float32)
    key_part = jnp.clip(key_part, -0.12, 0.12)
    query_part = query_spread * jax.random.normal(jax.random.fold_in(key, 12), (D, HEADS, 2, HEAD), jnp.float32)
    query_part = jnp.clip(query_part, -4.0, 4.0)
    return (query_part.reshape(D, HEADS * 2 * HEAD), key_part.reshape(D, HEADS * 2 * HEAD))


def draw_query_weight(key, part):
    return query_key_pair(key)[0].astype(jnp.bfloat16)


def draw_key_weight(key, part):
    return query_key_pair(key)[1].astype(jnp.bfloat16)


def steps_of(rng, extent, split, least, high):
    def one(dim, parts):
        heights = jax.random.uniform(jax.random.fold_in(jax.random.fold_in(rng, 6), dim), (parts,), jnp.float32, least / len(split), high / len(split))
        return jnp.repeat(jnp.exp(heights), extent[dim] // parts).reshape((-1,) + (1,) * (len(extent) - dim - 1))

    level = one(*split[0])
    for cut in split[1:]:
        level = level * one(*cut)
    return level


def noise(stream_key, dims, width, reach, shards=(), kind=jnp.bfloat16):
    result = jax.random.normal(stream_key, dims, jnp.float32) * width
    if len(shards) > 0:
        result = steps_of(stream_key, dims, shards, -0.22, 0.18) * result
    return jnp.clip(result, min=-reach, max=reach).astype(kind)


def setup_inputs(seed: int = 0) -> dict:
    key_of = jax.random.split(jax.random.key(seed), 14)
    return {
        "latent": noise(key_of[0], (SAMPLES, SEQ, D), 1.0, 6.0, ((0, 2), (1, 16))),
        "condition": noise(key_of[1], (SAMPLES, D), 1.0, 6.0, ((0, 2), (1, 16))),
        "context": noise(key_of[2], (SAMPLES, CTX, D), 1.0, 6.0, ((0, 2), (1, 4))),
        "context_vector": noise(key_of[3], (D,), 1.0, 6.0, ((0, 16),)),
        "modulator": noise(key_of[4], (D, 3 * D), (D // 6) ** -0.5, 0.3125, ((0, 16),)),
        "norm_gain": jnp.clip(1.0 + 0.18 * jax.random.normal(key_of[5], (D,), jnp.float32), 0.1, 1.9),
        "query_weight": draw_query_weight(jax.random.fold_in(key_of[13], 71), 0),
        "key_weight": draw_key_weight(jax.random.fold_in(key_of[13], 71), 0),
        "value_weight": noise(key_of[8], (D, 2 * HEAD * HEADS), D ** -0.5, 0.125, ((1, 4),)),
        "head_gain": jnp.clip(1.0 + 0.18 * jax.random.normal(key_of[9], (2 * HEAD,), jnp.float32), 0.1, 1.9),
        "lambdas": jnp.clip(0.3 + 0.5 * jax.random.uniform(key_of[10], (HEADS,), jnp.float32) ** steps_of(key_of[10], (HEADS,), ((0, 4),), -0.2, 0.2), 0.3, 0.8),
        "context_bias": jnp.clip(1.3 + 1.4000001 * jax.random.uniform(key_of[11], (HEADS, 2), jnp.float32) ** steps_of(key_of[11], (HEADS, 2), ((0, 4),), -0.2, 0.2), 1.3, 2.7),
        "out_weight": noise(key_of[12], (2 * HEAD * HEADS, D), (2 * HEAD * HEADS) ** -0.5, 0.25, ((0, 4),)),
    }


EPSILON = 1e-06
OUT_SCALE = 0.8

def modulate(inputs, gain_vector, shift_vector, scale_vector):
    as_float = inputs.astype(jnp.float32)
    normed = as_float * lax.rsqrt(lax.optimization_barrier(jnp.mean(as_float * as_float, axis=-1, keepdims=True)) + EPSILON)
    return (normed * gain_vector * (1.0 + scale_vector) + shift_vector).astype(jnp.bfloat16)

def reference(latent, condition, context, context_vector, modulator, norm_gain, query_weight, key_weight, value_weight, head_gain, lambdas, context_bias, out_weight):
    activated = jax.nn.silu(jnp.concatenate([condition, context_vector[None, :]], axis=0).astype(jnp.float32))
    activated = activated.astype(jnp.bfloat16)
    modulations = jnp.dot(activated, modulator, preferred_element_type=jnp.float32)
    ctx_shift = modulations[SAMPLES, :D]
    ctx_scale = modulations[SAMPLES, D:2 * D]
    block_rows = math.gcd(SEQ, 512)
    key_flags = jnp.concatenate([jnp.zeros((SEQ,), jnp.float32), jnp.ones((CTX,), jnp.float32)])
    key_bias = context_bias[:, :, None, None] * key_flags
    results = []
    for sample_index in range(SAMPLES):
        shift_vector = modulations[sample_index, :D]
        scale_vector = modulations[sample_index, D:2 * D]
        gate_vector = modulations[sample_index, 2 * D:]
        hidden = modulate(latent[sample_index], norm_gain, shift_vector, scale_vector)
        ctx_hidden = modulate(context[sample_index], norm_gain, ctx_shift, ctx_scale)
        queries = jnp.dot(hidden, query_weight, preferred_element_type=jnp.float32).astype(jnp.bfloat16)
        queries = queries.reshape(SEQ, HEADS, 2, HEAD)
        all_keys = jnp.concatenate([jnp.dot(hidden, key_weight, preferred_element_type=jnp.float32).astype(jnp.bfloat16), jnp.dot(ctx_hidden, key_weight, preferred_element_type=jnp.float32).astype(jnp.bfloat16)], axis=0)
        all_values = jnp.concatenate([jnp.dot(hidden, value_weight, preferred_element_type=jnp.float32).astype(jnp.bfloat16), jnp.dot(ctx_hidden, value_weight, preferred_element_type=jnp.float32).astype(jnp.bfloat16)], axis=0)
        keys_float = all_keys.reshape(SEQ + CTX, HEADS, 2, HEAD).astype(jnp.float32)
        values_float = all_values.reshape(SEQ + CTX, HEADS, 2 * HEAD).astype(jnp.float32)

        def attend(query_block):
            scores = jnp.einsum('qhmd,khmd->hmqk', query_block.astype(jnp.float32), keys_float) * HEAD ** (-0.5)
            scores = scores + key_bias
            row_max = lax.optimization_barrier(jnp.max(scores, axis=-1, keepdims=True))
            weights = jnp.exp(scores - row_max)
            totals = lax.optimization_barrier(jnp.sum(weights, axis=-1))
            rounded = lax.optimization_barrier(weights.astype(jnp.bfloat16)).astype(jnp.float32)
            summed = jnp.einsum('hmqk,khe->hmqe', rounded, values_float)
            mixed = summed[:, 0] / totals[:, 0, :, None] - lambdas[:, None, None] * summed[:, 1] / totals[:, 1, :, None]
            normed = mixed * lax.rsqrt(lax.optimization_barrier(jnp.mean(mixed * mixed, axis=-1, keepdims=True)) + EPSILON) * head_gain * OUT_SCALE
            return jnp.transpose(normed, (1, 0, 2)).reshape(block_rows, HEADS * 2 * HEAD).astype(jnp.bfloat16)
        query_blocks = queries.reshape(SEQ // block_rows, block_rows, HEADS, 2, HEAD)
        attended = lax.map(attend, query_blocks).reshape(SEQ, HEADS * 2 * HEAD)
        branch = jnp.dot(attended, out_weight, preferred_element_type=jnp.float32)
        results.append((latent[sample_index].astype(jnp.float32) + gate_vector * branch).astype(jnp.bfloat16))
    return jnp.stack(results)
```

```python
import functools

import jax
import jax.numpy as jnp
from jax import lax
from jax.experimental import pallas as pl
from jax.experimental.pallas import tpu as pltpu
from jax.sharding import PartitionSpec as P

EPSILON = 1e-06
OUT_SCALE = 0.8
KEY_BLOCK = 2048
LOW_START = -1e30


def modulate(inputs, gain_vector, shift_vector, scale_vector):
    as_float = inputs.astype(jnp.float32)
    normed = as_float * lax.rsqrt(jnp.mean(as_float * as_float, axis=-1, keepdims=True) + EPSILON)
    return (normed * gain_vector * (1.0 + scale_vector) + shift_vector).astype(jnp.bfloat16)


def fold_block(running, queries, keys_in, values_in, key_flags, bias_table, score_scale):
    run_max, run_total, summed = running
    scores = (
        jnp.einsum("qhmd,khmd->hmqk", queries, keys_in, preferred_element_type=jnp.float32)
        * score_scale
    )
    if key_flags is not None:
        scores = scores + bias_table[:, :, None, None] * key_flags
    new_max = jnp.maximum(run_max, jnp.max(scores, axis=-1))
    shrink = jnp.exp(run_max - new_max)
    weights = jnp.exp(scores - new_max[..., None])
    run_total = run_total * shrink + jnp.sum(weights, axis=-1)
    summed = summed * shrink[..., None] + jnp.einsum(
        "hmqk,khe->hmqe",
        weights.astype(jnp.bfloat16),
        values_in,
        preferred_element_type=jnp.float32,
    )
    return (new_max, run_total, summed)


def fold_keys(running, queries, keys_in, values_in, key_flags, bias_table, score_scale):
    full_blocks = keys_in.shape[0] // KEY_BLOCK
    if full_blocks > 1:
        edge = full_blocks * KEY_BLOCK
        stacked = (
            keys_in[:edge].reshape((full_blocks, KEY_BLOCK) + keys_in.shape[1:]),
            values_in[:edge].reshape((full_blocks, KEY_BLOCK) + values_in.shape[1:]),
        )
        if key_flags is not None:
            stacked = stacked + (key_flags[:edge].reshape(full_blocks, KEY_BLOCK),)

        def fold_step(current, block_data):
            flag_part = None if key_flags is None else block_data[2]
            return (
                fold_block(
                    current,
                    queries,
                    block_data[0],
                    block_data[1],
                    flag_part,
                    bias_table,
                    score_scale,
                ),
                None,
            )

        running, ignored = lax.scan(fold_step, running, stacked)
        keys_in = keys_in[edge:]
        values_in = values_in[edge:]
        key_flags = None if key_flags is None else key_flags[edge:]
    if keys_in.shape[0] > 0:
        running = fold_block(
            running, queries, keys_in, values_in, key_flags, bias_table, score_scale
        )
    return running


def body(
    latent,
    condition,
    context,
    context_vector,
    modulator,
    norm_gain,
    query_weight,
    key_weight,
    value_weight,
    head_gain,
    lambdas,
    context_bias,
    out_weight,
):
    model_width = latent.shape[2]
    local_heads = lambdas.shape[0]
    query_width = query_weight.shape[1]
    head_size = query_width // (2 * local_heads)
    value_size = value_weight.shape[1] // local_heads
    score_scale = head_size ** (-0.5)
    activated = jax.nn.silu(
        jnp.concatenate([condition, context_vector[None, :]], axis=0).astype(jnp.float32)
    )
    partial_terms = jnp.dot(
        activated.astype(jnp.bfloat16), modulator, preferred_element_type=jnp.float32
    )
    modulations = lax.psum(partial_terms, ("sp", "tp"))
    hidden = modulate(
        latent[0],
        norm_gain,
        modulations[0, :model_width],
        modulations[0, model_width : 2 * model_width],
    )
    ctx_hidden = modulate(
        context[0],
        norm_gain,
        modulations[1, :model_width],
        modulations[1, model_width : 2 * model_width],
    )
    gate_vector = modulations[0, 2 * model_width :]
    incoming = lax.all_gather(hidden, "tp", axis=0, tiled=True)
    projected = jnp.concatenate(
        [
            jnp.dot(incoming, query_weight, preferred_element_type=jnp.float32),
            jnp.dot(incoming, key_weight, preferred_element_type=jnp.float32),
            jnp.dot(incoming, value_weight, preferred_element_type=jnp.float32),
        ],
        axis=1,
    ).astype(jnp.bfloat16)
    query_rows = projected.shape[0]
    queries = projected[:, :query_width].reshape(query_rows, local_heads, 2, head_size)
    own_keys = projected[:, query_width : 2 * query_width]
    own_values = projected[:, 2 * query_width :]
    gathered_context = lax.all_gather(ctx_hidden, "sp", axis=0, tiled=True)
    ctx_keys = jnp.dot(gathered_context, key_weight, preferred_element_type=jnp.float32).astype(
        jnp.bfloat16
    )
    ctx_values = jnp.dot(gathered_context, value_weight, preferred_element_type=jnp.float32).astype(
        jnp.bfloat16
    )
    start_carry = (
        jnp.full((local_heads, 2, query_rows), LOW_START, jnp.float32),
        jnp.zeros((local_heads, 2, query_rows), jnp.float32),
        jnp.zeros((local_heads, 2, query_rows, value_size), jnp.float32),
    )
    pieces = (own_keys, own_values)
    initial = fold_keys(
        start_carry,
        queries,
        ctx_keys.reshape(-1, local_heads, 2, head_size),
        ctx_values.reshape(-1, local_heads, value_size),
        jnp.ones((ctx_keys.shape[0],), jnp.float32),
        context_bias,
        score_scale,
    )
    incoming = (
        lax.all_gather(pieces[0], "sp", axis=0, tiled=True),
        lax.all_gather(pieces[1], "sp", axis=0, tiled=True),
    )
    run_max, run_total, summed = fold_keys(
        initial,
        queries,
        incoming[0].reshape(-1, local_heads, 2, head_size),
        incoming[1].reshape(-1, local_heads, value_size),
        None,
        context_bias,
        score_scale,
    )
    mixed = (
        summed[:, 0] / run_total[:, 0, :, None]
        - lambdas[:, None, None] * summed[:, 1] / run_total[:, 1, :, None]
    )
    normed = (
        mixed
        * lax.rsqrt(jnp.mean(mixed * mixed, axis=-1, keepdims=True) + EPSILON)
        * head_gain
        * OUT_SCALE
    )
    attended = (
        jnp.transpose(normed, (1, 0, 2))
        .reshape(query_rows, local_heads * value_size)
        .astype(jnp.bfloat16)
    )
    exchanged = lax.all_to_all(attended, "tp", split_axis=0, concat_axis=1, tiled=True)
    whole_weight = lax.all_gather(out_weight, "tp", axis=0, tiled=True)
    branch = jnp.dot(exchanged, whole_weight, preferred_element_type=jnp.float32)
    result = (latent[0].astype(jnp.float32) + gate_vector * branch).astype(jnp.bfloat16)
    return result[None]


MESH = pl.DeviceIdType.MESH
LANES = 128


def fused_kernel(
    sp_n, tp_n, score_scale,
    latent, condition, context, context_vector, modulator, norm_gain,
    query_weight, key_weight, value_weight, head_gain, lambdas, context_bias, out_weight,
    out,
    mod_v, part, rs_in, mods, lat, ctx_all, w_q, w_kv, w_out, vecs, hid, kvb, att_out, att_in,
    own_sem, rs_ss, rs_rs, ag_ss, ag_rs, lat_ss, lat_rs, ctx_ss, ctx_rs,
    kv_os, kv_ss, kv_rs, wt_ss, wt_rs, wd_ss, wd_rs, at_ss, at_rs,
):
    sp = lax.axis_index("sp")
    tp = lax.axis_index("tp")
    dp = lax.axis_index("dp")
    n = sp_n * tp_n
    rank = sp * tp_n + tp
    half = lat.shape[1]
    width = lat.shape[2]
    rows = half * 2
    qrows = rows * tp_n
    chunk = part.shape[2]

    barrier = pltpu.get_barrier_semaphore()

    def greet(d, carry):
        peer = lax.rem(rank + d, n)
        pl.semaphore_signal(
            barrier, inc=1, device_id=(peer // tp_n, lax.rem(peer, tp_n), dp), device_id_type=MESH
        )
        return carry

    lax.fori_loop(1, n, greet, 0)
    pl.semaphore_signal(barrier, inc=1, device_id=(sp, tp, 1 - dp), device_id_type=MESH)

    loads = [
        pltpu.make_async_copy(modulator, mod_v, own_sem.at[0]),
        pltpu.make_async_copy(latent, lat.at[pl.ds(tp * 2, 2)], own_sem.at[1]),
        pltpu.make_async_copy(key_weight, w_kv.at[:, pl.ds(0, LANES)], own_sem.at[2]),
        pltpu.make_async_copy(value_weight, w_kv.at[:, pl.ds(LANES, LANES)], own_sem.at[3]),
        pltpu.make_async_copy(query_weight, w_q, own_sem.at[4]),
        pltpu.make_async_copy(out_weight, w_out.at[pl.ds(tp * 4, 4)], own_sem.at[5]),
    ]
    for load in loads:
        load.start()

    rows_in = jnp.concatenate([condition[...], context_vector[...]], axis=0).astype(jnp.float32)
    activated = jax.nn.silu(rows_in).astype(jnp.bfloat16)
    loads[0].wait()
    partial_terms = jnp.dot(activated, mod_v[...], preferred_element_type=jnp.float32)
    for p in range(n):
        part[p] = partial_terms[:, p * chunk : (p + 1) * chunk]
    loads[1].wait()
    pl.semaphore_wait(barrier, n)

    def rs_copy(d):
        peer = lax.rem(rank + d, n)
        return pltpu.make_async_remote_copy(
            src_ref=part.at[peer], dst_ref=rs_in.at[d], send_sem=rs_ss.at[d], recv_sem=rs_rs.at[d],
            device_id=(peer // tp_n, lax.rem(peer, tp_n), dp), device_id_type=MESH,
        )

    def ag_copy(d):
        peer = lax.rem(rank + d, n)
        return pltpu.make_async_remote_copy(
            src_ref=mods.at[rank], dst_ref=mods.at[rank], send_sem=ag_ss.at[d], recv_sem=ag_rs.at[d],
            device_id=(peer // tp_n, lax.rem(peer, tp_n), dp), device_id_type=MESH,
        )

    def ag_arrival(d):
        peer = lax.rem(rank - d + n, n)
        return pltpu.make_async_remote_copy(
            src_ref=mods.at[peer], dst_ref=mods.at[peer], send_sem=ag_ss.at[d], recv_sem=ag_rs.at[d],
            device_id=(peer // tp_n, lax.rem(peer, tp_n), dp), device_id_type=MESH,
        )

    def each(first, last, act):
        def step(d, carry):
            act(d)
            return carry

        lax.fori_loop(first, last, step, 0)

    each(1, n, lambda d: rs_copy(d).start())

    across = tp + 1 - 2 * lax.rem(tp, 2)
    along = lax.rem(tp + 2, 4)
    corner = along + 1 - 2 * lax.rem(along, 2)

    class Plane:
        def __init__(self, buf, index, ss, rs):
            self.buf, self.index, self.ss, self.rs = buf, index, ss, rs

        def copy(self, owner, part_no, target, slot, kind):
            place = self.buf.at[self.index(owner, part_no)]
            return pltpu.make_async_remote_copy(
                src_ref=place, dst_ref=place, send_sem=self.ss.at[slot],
                recv_sem=self.rs.at[kind * 2 + part_no],
                device_id=(sp, target, dp), device_id_type=MESH,
            )

        def first(self):
            return [
                self.copy(tp, 0, across, 0, 0),
                self.copy(tp, 1, along, 1, 1),
                self.copy(tp, 1, across, 2, 0),
                self.copy(tp, 0, along, 3, 1),
            ]

        def relays(self):
            return [self.copy(across, 0, along, 4, 2), self.copy(along, 1, across, 5, 2)]

        def arrival(self, kind, part_no):
            owner = (across, along, corner)[kind]
            return self.copy(owner, part_no, across, 0, kind)

    plane = Plane(lat, lambda o, q: o * 2 + q, lat_ss, lat_rs)
    lat_first = plane.first()
    for copy in lat_first:
        copy.start()

    def ctx_copy(d):
        peer = lax.rem(sp + d, sp_n)
        return pltpu.make_async_remote_copy(
            src_ref=context, dst_ref=ctx_all.at[sp], send_sem=ctx_ss.at[d], recv_sem=ctx_rs.at[d],
            device_id=(peer, tp, dp), device_id_type=MESH,
        )

    def ctx_arrival(d):
        peer = lax.rem(sp - d + sp_n, sp_n)
        return pltpu.make_async_remote_copy(
            src_ref=context, dst_ref=ctx_all.at[peer], send_sem=ctx_ss.at[d], recv_sem=ctx_rs.at[d],
            device_id=(peer, tp, dp), device_id_type=MESH,
        )

    for d in range(1, sp_n):
        ctx_copy(d).start()
    ctx_all[sp] = context[...]
    rs_in[0] = part[rank]

    each(1, n, lambda d: rs_copy(d).wait_recv())
    total = rs_in[0]
    for d in range(1, n):
        total = total + rs_in[d]
    mods[rank] = total
    each(1, n, lambda d: ag_copy(d).start())

    lat_relays = plane.relays()
    plane.arrival(0, 0).wait_recv()
    lat_relays[0].start()
    plane.arrival(1, 1).wait_recv()
    lat_relays[1].start()

    for d in range(1, sp_n):
        ctx_arrival(d).wait_recv()
    each(1, n, lambda d: ag_arrival(d).wait_recv())
    whole = jnp.concatenate([mods[p] for p in range(n)], axis=1)
    gain = norm_gain[...]
    vecs[0:1, :] = gain * (1.0 + whole[0:1, width : 2 * width])
    vecs[1:2, :] = whole[0:1, :width]
    vecs[2:3, :] = gain * (1.0 + whole[1:2, width : 2 * width])
    vecs[3:4, :] = whole[1:2, :width]
    vecs[4:5, :] = whole[0:1, 2 * width :]

    def normed_rows(x, at):
        x = x.astype(jnp.float32)
        scale = lax.rsqrt(jnp.mean(x * x, axis=-1, keepdims=True) + EPSILON)
        return (x * scale * vecs[at : at + 1, :] + vecs[at + 1 : at + 2, :]).astype(jnp.bfloat16)

    def norm_block(owner):
        for q in range(2):
            at = pl.multiple_of((owner * 2 + q) * half, half)
            hid[pl.ds(at, half), :] = normed_rows(lat[owner * 2 + q], 0)

    ctx_rows = ctx_all.shape[0] * ctx_all.shape[1]
    hid[qrows : qrows + ctx_rows, :] = normed_rows(
        ctx_all[...].astype(jnp.float32).reshape(ctx_rows, width), 2
    )
    norm_block(tp)
    plane.arrival(0, 1).wait_recv()
    norm_block(across)
    plane.arrival(1, 0).wait_recv()
    norm_block(along)
    plane.arrival(2, 0).wait_recv()
    plane.arrival(2, 1).wait_recv()
    norm_block(corner)

    for load in loads[2:]:
        load.wait()
    kv = jnp.dot(hid[...], w_kv[...], preferred_element_type=jnp.float32).astype(jnp.bfloat16)
    kvb[sp] = kv[:qrows]
    ctx_kv = kv[qrows:]

    def kv_own(to, slot):
        return pltpu.make_async_remote_copy(
            src_ref=kvb.at[sp], dst_ref=kvb.at[sp], send_sem=kv_os.at[slot], recv_sem=kv_rs.at[sp],
            device_id=(to, tp, dp), device_id_type=MESH,
        )

    @pl.when(sp + 1 < sp_n)
    def _():
        kv_own(sp + 1, 0).start()

    @pl.when(sp > 0)
    def _():
        kv_own(sp - 1, 1).start()

    wplane = Plane(w_out, lambda o, q: o * 4 + dp * 2 + q, wt_ss, wt_rs)
    w_first = wplane.first()
    for copy in w_first:
        copy.start()

    queries = jnp.dot(hid[:qrows, :], w_q[...], preferred_element_type=jnp.float32) * score_scale
    queries = queries.astype(jnp.bfloat16)
    head = queries.shape[1] // 2
    lane = lax.broadcasted_iota(jnp.int32, queries.shape, 1)
    zero = jnp.zeros_like(queries)
    both = jnp.concatenate(
        [jnp.where(lane < head, queries, zero), jnp.where(lane < head, zero, queries)], axis=0
    )

    def score(keys):
        return lax.dot_general(
            both, keys, (((1,), (1,)), ((), ())), preferred_element_type=jnp.float32
        )

    map_row = lax.broadcasted_iota(jnp.int32, (2 * qrows, 1), 0)
    bias = jnp.where(map_row < qrows, context_bias[0, 0], context_bias[0, 1])

    def fold(running, scores, values):
        top = jnp.max(scores, axis=-1, keepdims=True)
        if running is not None:
            top = jnp.maximum(running[0], top)
        weights = jnp.exp(scores - top)
        count = jnp.sum(weights, axis=-1, keepdims=True)
        summed = jnp.dot(weights.astype(jnp.bfloat16), values, preferred_element_type=jnp.float32)
        if running is not None:
            shrink = jnp.exp(running[0] - top)
            count = running[1] * shrink + count
            summed = running[2] * shrink + summed
        return top, count, summed

    running = fold(None, score(ctx_kv[:, :LANES]) + bias, ctx_kv[:, LANES:])
    running = fold(running, score(kv[:qrows, :LANES]), kv[:qrows, LANES:])

    w_relays = wplane.relays()
    wplane.arrival(0, 0).wait_recv()
    w_relays[0].start()
    wplane.arrival(1, 1).wait_recv()
    w_relays[1].start()

    high = (2 * sp) // sp_n

    def block_at(t):
        up = (t - 1) + jnp.where(t - 1 >= sp, 1, 0)
        down = (sp_n - t) - jnp.where(sp_n - t <= sp, 1, 0)
        return jnp.where(high == 0, up, down)

    def onward(b):
        step = jnp.where(b < sp, 1, -1)
        to = sp + step
        ok = jnp.logical_and(to >= 0, to < sp_n)
        safe = jnp.where(ok, to, sp - step)
        return ok, pltpu.make_async_remote_copy(
            src_ref=kvb.at[b], dst_ref=kvb.at[b], send_sem=kv_ss.at[b], recv_sem=kv_rs.at[b],
            device_id=(safe, tp, dp), device_id_type=MESH,
        )

    def sibling(owner, part_no, slot):
        place = w_out.at[owner * 4 + dp * 2 + part_no]
        return pltpu.make_async_remote_copy(
            src_ref=place, dst_ref=place, send_sem=wd_ss.at[slot], recv_sem=wd_rs.at[slot],
            device_id=(sp, tp, 1 - dp), device_id_type=MESH,
        )

    def sibling_arrival(owner, part_no, slot):
        place = w_out.at[owner * 4 + (1 - dp) * 2 + part_no]
        return pltpu.make_async_remote_copy(
            src_ref=place, dst_ref=place, send_sem=wd_ss.at[slot], recv_sem=wd_rs.at[slot],
            device_id=(sp, tp, 1 - dp), device_id_type=MESH,
        )

    owners = (across, along, corner)
    sent = []
    for t in range(1, sp_n):
        b = block_at(t)
        ok, copy = onward(b)
        copy.wait_recv()
        pl.when(ok)(copy.start)
        sent.append((ok, copy))
        running = fold(running, score(kvb[b, :, :LANES]), kvb[b, :, LANES:])

    top, count, summed = running
    shares = summed / count
    mixed = shares[:qrows] - lambdas[0] * shares[qrows:]
    normed = (
        mixed
        * lax.rsqrt(jnp.mean(mixed * mixed, axis=-1, keepdims=True) + EPSILON)
        * head_gain[...]
        * OUT_SCALE
    ).astype(jnp.bfloat16)
    for p in range(tp_n):
        att_out[p] = normed[p * rows : (p + 1) * rows]

    def at_copy(d):
        peer = lax.rem(tp + d, tp_n)
        return pltpu.make_async_remote_copy(
            src_ref=att_out.at[peer], dst_ref=att_in.at[tp], send_sem=at_ss.at[d], recv_sem=at_rs.at[d],
            device_id=(sp, peer, dp), device_id_type=MESH,
        )

    def at_arrival(d):
        peer = lax.rem(tp - d + tp_n, tp_n)
        return pltpu.make_async_remote_copy(
            src_ref=att_out.at[peer], dst_ref=att_in.at[peer], send_sem=at_ss.at[d], recv_sem=at_rs.at[d],
            device_id=(sp, peer, dp), device_id_type=MESH,
        )

    for d in range(1, tp_n):
        at_copy(d).start()
    att_in[tp] = att_out[tp]

    w_sent = []
    for kind, part_no in ((0, 0), (1, 1), (0, 1), (1, 0), (2, 0), (2, 1)):
        if (kind, part_no) not in ((0, 0), (1, 1)):
            wplane.arrival(kind, part_no).wait_recv()
        copy = sibling(owners[kind], part_no, kind * 2 + part_no)
        copy.start()
        w_sent.append(copy)
    for kind in range(3):
        for part_no in range(2):
            sibling_arrival(owners[kind], part_no, kind * 2 + part_no).wait_recv()
    for d in range(1, tp_n):
        at_arrival(d).wait_recv()

    attended = jnp.concatenate([att_in[p] for p in range(tp_n)], axis=1)
    step = 512
    for first in range(0, width, step):
        cols = slice(first, first + step)
        weight = w_out[:, :, cols].reshape(attended.shape[1], step)
        branch = jnp.dot(attended, weight, preferred_element_type=jnp.float32)
        for q in range(2):
            mine = lat[tp * 2 + q, :, cols].astype(jnp.float32)
            update = mine + vecs[4:5, cols] * branch[q * half : (q + 1) * half]
            out[q * half : (q + 1) * half, cols] = update.astype(jnp.bfloat16)

    each(1, n, lambda d: rs_copy(d).wait_send())
    each(1, n, lambda d: ag_copy(d).wait_send())
    for copy in lat_first + lat_relays + w_first + w_relays + w_sent:
        copy.wait_send()
    for d in range(1, sp_n):
        ctx_copy(d).wait_send()
    pl.when(sp + 1 < sp_n)(lambda: kv_own(sp + 1, 0).wait_send())
    pl.when(sp > 0)(lambda: kv_own(sp - 1, 1).wait_send())
    for ok, copy in sent:
        pl.when(ok)(copy.wait_send)
    for d in range(1, tp_n):
        at_copy(d).wait_send()


def fused(
    axes, latent, condition, context, context_vector, modulator, norm_gain, query_weight,
    key_weight, value_weight, head_gain, lambdas, context_bias, out_weight,
):
    sp_n, tp_n, dp_n = axes
    n = sp_n * tp_n
    rows, width = latent.shape[1:]
    half = rows // 2
    chunk = modulator.shape[1] // n
    ctx_rows = context.shape[1]
    qw = query_weight.shape[1]
    value = value_weight.shape[1]
    qrows = rows * tp_n
    wrows = out_weight.shape[0] // 4
    bf, f32 = jnp.bfloat16, jnp.float32
    vm = pl.BlockSpec(memory_space=pltpu.VMEM)
    sm = pl.BlockSpec(memory_space=pltpu.SMEM)
    hb = pl.BlockSpec(memory_space=pl.ANY)
    dma = lambda k: pltpu.SemaphoreType.DMA((k,))
    result = pl.pallas_call(
        functools.partial(fused_kernel, sp_n, tp_n, (qw // 2) ** (-0.5)),
        out_shape=jax.ShapeDtypeStruct((rows, width), bf),
        in_specs=[hb, vm, vm, vm, hb, vm, hb, hb, hb, vm, sm, sm, hb],
        out_specs=vm,
        scratch_shapes=[
            pltpu.VMEM(modulator.shape, bf),
            pltpu.VMEM((n, 2, chunk), f32),
            pltpu.VMEM((n, 2, chunk), f32),
            pltpu.VMEM((n, 2, chunk), f32),
            pltpu.VMEM((tp_n * 2, half, width), bf),
            pltpu.VMEM((sp_n, ctx_rows, width), bf),
            pltpu.VMEM((width, qw), bf),
            pltpu.VMEM((width, qw + value), bf),
            pltpu.VMEM((tp_n * 4, wrows, width), bf),
            pltpu.VMEM((8, width), f32),
            pltpu.VMEM((qrows + sp_n * ctx_rows, width), bf),
            pltpu.VMEM((sp_n, qrows, qw + value), bf),
            pltpu.VMEM((tp_n, rows, value), bf),
            pltpu.VMEM((tp_n, rows, value), bf),
            dma(6), dma(n), dma(n), dma(n), dma(n), dma(6), dma(6), dma(sp_n), dma(sp_n),
            dma(2), dma(sp_n), dma(sp_n), dma(6), dma(6), dma(6), dma(6), dma(tp_n), dma(tp_n),
        ],
        compiler_params=pltpu.CompilerParams(
            collective_id=0, has_side_effects=True, vmem_limit_bytes=48 * 2**20
        ),
        name="fused_block",
    )(
        latent.reshape(2, half, width),
        condition,
        context[0],
        context_vector[None, :],
        modulator,
        norm_gain[None, :],
        query_weight,
        key_weight,
        value_weight,
        head_gain[None, :],
        lambdas,
        context_bias,
        out_weight.reshape(4, wrows, width),
    )
    return result[None]


def choose(axes, *arrays):
    sp_n, tp_n, dp_n = axes
    latent, modulator, query_weight, value_weight = arrays[0], arrays[4], arrays[6], arrays[8]
    lambdas, out_weight = arrays[10], arrays[12]
    fits = (
        tp_n == 4
        and dp_n == 2
        and 1 < sp_n <= 8
        and lambdas.shape[0] == 1
        and query_weight.shape[1] == LANES
        and value_weight.shape[1] == LANES
        and modulator.shape[1] % (sp_n * tp_n * LANES) == 0
        and latent.shape[1] % 32 == 0
        and latent.shape[2] % 512 == 0
        and out_weight.shape[0] % 64 == 0
    )
    return fused(axes, *arrays) if fits else body(*arrays)


def solution(mesh):
    placed = (
        P("dp", ("sp", "tp"), None),
        P("dp", ("sp", "tp")),
        P("dp", "sp", None),
        P(("sp", "tp")),
        P(("sp", "tp"), None),
        P(),
        P(None, "tp"),
        P(None, "tp"),
        P(None, "tp"),
        P(),
        P("tp"),
        P("tp", None),
        P("tp", None),
    )
    axes = (mesh.shape["sp"], mesh.shape["tp"], mesh.shape["dp"])
    return jax.shard_map(
        functools.partial(choose, axes), mesh=mesh, in_specs=placed, out_specs=P("dp", ("sp", "tp"), None), check_vma=False
    )
```

```python
import functools

import jax
import jax.numpy as jnp
from jax import lax
from jax.experimental import pallas as pl
from jax.experimental.pallas import tpu as pltpu
from jax.sharding import PartitionSpec as P

EPSILON = 1e-06
OUT_SCALE = 0.8
KEY_BLOCK = 2048
LOW_START = -1e30


def modulate(inputs, gain_vector, shift_vector, scale_vector):
    as_float = inputs.astype(jnp.float32)
    normed = as_float * lax.rsqrt(jnp.mean(as_float * as_float, axis=-1, keepdims=True) + EPSILON)
    return (normed * gain_vector * (1.0 + scale_vector) + shift_vector).astype(jnp.bfloat16)


def fold_block(running, queries, keys_in, values_in, key_flags, bias_table, score_scale):
    run_max, run_total, summed = running
    scores = (
        jnp.einsum("qhmd,khmd->hmqk", queries, keys_in, preferred_element_type=jnp.float32)
        * score_scale
    )
    if key_flags is not None:
        scores = scores + bias_table[:, :, None, None] * key_flags
    new_max = jnp.maximum(run_max, jnp.max(scores, axis=-1))
    shrink = jnp.exp(run_max - new_max)
    weights = jnp.exp(scores - new_max[..., None])
    run_total = run_total * shrink + jnp.sum(weights, axis=-1)
    summed = summed * shrink[..., None] + jnp.einsum(
        "hmqk,khe->hmqe",
        weights.astype(jnp.bfloat16),
        values_in,
        preferred_element_type=jnp.float32,
    )
    return (new_max, run_total, summed)


def fold_keys(running, queries, keys_in, values_in, key_flags, bias_table, score_scale):
    full_blocks = keys_in.shape[0] // KEY_BLOCK
    if full_blocks > 1:
        edge = full_blocks * KEY_BLOCK
        stacked = (
            keys_in[:edge].reshape((full_blocks, KEY_BLOCK) + keys_in.shape[1:]),
            values_in[:edge].reshape((full_blocks, KEY_BLOCK) + values_in.shape[1:]),
        )
        if key_flags is not None:
            stacked = stacked + (key_flags[:edge].reshape(full_blocks, KEY_BLOCK),)

        def fold_step(current, block_data):
            flag_part = None if key_flags is None else block_data[2]
            return (
                fold_block(
                    current,
                    queries,
                    block_data[0],
                    block_data[1],
                    flag_part,
                    bias_table,
                    score_scale,
                ),
                None,
            )

        running, ignored = lax.scan(fold_step, running, stacked)
        keys_in = keys_in[edge:]
        values_in = values_in[edge:]
        key_flags = None if key_flags is None else key_flags[edge:]
    if keys_in.shape[0] > 0:
        running = fold_block(
            running, queries, keys_in, values_in, key_flags, bias_table, score_scale
        )
    return running


def body(
    latent,
    condition,
    context,
    context_vector,
    modulator,
    norm_gain,
    query_weight,
    key_weight,
    value_weight,
    head_gain,
    lambdas,
    context_bias,
    out_weight,
):
    model_width = latent.shape[2]
    local_heads = lambdas.shape[0]
    query_width = query_weight.shape[1]
    head_size = query_width // (2 * local_heads)
    value_size = value_weight.shape[1] // local_heads
    score_scale = head_size ** (-0.5)
    activated = jax.nn.silu(
        jnp.concatenate([condition, context_vector[None, :]], axis=0).astype(jnp.float32)
    )
    partial_terms = jnp.dot(
        activated.astype(jnp.bfloat16), modulator, preferred_element_type=jnp.float32
    )
    modulations = lax.psum(partial_terms, ("sp", "tp"))
    hidden = modulate(
        latent[0],
        norm_gain,
        modulations[0, :model_width],
        modulations[0, model_width : 2 * model_width],
    )
    ctx_hidden = modulate(
        context[0],
        norm_gain,
        modulations[1, :model_width],
        modulations[1, model_width : 2 * model_width],
    )
    gate_vector = modulations[0, 2 * model_width :]
    incoming = lax.all_gather(hidden, "tp", axis=0, tiled=True)
    projected = jnp.concatenate(
        [
            jnp.dot(incoming, query_weight, preferred_element_type=jnp.float32),
            jnp.dot(incoming, key_weight, preferred_element_type=jnp.float32),
            jnp.dot(incoming, value_weight, preferred_element_type=jnp.float32),
        ],
        axis=1,
    ).astype(jnp.bfloat16)
    query_rows = projected.shape[0]
    queries = projected[:, :query_width].reshape(query_rows, local_heads, 2, head_size)
    own_keys = projected[:, query_width : 2 * query_width]
    own_values = projected[:, 2 * query_width :]
    gathered_context = lax.all_gather(ctx_hidden, "sp", axis=0, tiled=True)
    ctx_keys = jnp.dot(gathered_context, key_weight, preferred_element_type=jnp.float32).astype(
        jnp.bfloat16
    )
    ctx_values = jnp.dot(gathered_context, value_weight, preferred_element_type=jnp.float32).astype(
        jnp.bfloat16
    )
    start_carry = (
        jnp.full((local_heads, 2, query_rows), LOW_START, jnp.float32),
        jnp.zeros((local_heads, 2, query_rows), jnp.float32),
        jnp.zeros((local_heads, 2, query_rows, value_size), jnp.float32),
    )
    pieces = (own_keys, own_values)
    initial = fold_keys(
        start_carry,
        queries,
        ctx_keys.reshape(-1, local_heads, 2, head_size),
        ctx_values.reshape(-1, local_heads, value_size),
        jnp.ones((ctx_keys.shape[0],), jnp.float32),
        context_bias,
        score_scale,
    )
    incoming = (
        lax.all_gather(pieces[0], "sp", axis=0, tiled=True),
        lax.all_gather(pieces[1], "sp", axis=0, tiled=True),
    )
    run_max, run_total, summed = fold_keys(
        initial,
        queries,
        incoming[0].reshape(-1, local_heads, 2, head_size),
        incoming[1].reshape(-1, local_heads, value_size),
        None,
        context_bias,
        score_scale,
    )
    mixed = (
        summed[:, 0] / run_total[:, 0, :, None]
        - lambdas[:, None, None] * summed[:, 1] / run_total[:, 1, :, None]
    )
    normed = (
        mixed
        * lax.rsqrt(jnp.mean(mixed * mixed, axis=-1, keepdims=True) + EPSILON)
        * head_gain
        * OUT_SCALE
    )
    attended = (
        jnp.transpose(normed, (1, 0, 2))
        .reshape(query_rows, local_heads * value_size)
        .astype(jnp.bfloat16)
    )
    exchanged = lax.all_to_all(attended, "tp", split_axis=0, concat_axis=1, tiled=True)
    whole_weight = lax.all_gather(out_weight, "tp", axis=0, tiled=True)
    branch = jnp.dot(exchanged, whole_weight, preferred_element_type=jnp.float32)
    result = (latent[0].astype(jnp.float32) + gate_vector * branch).astype(jnp.bfloat16)
    return result[None]


MESH = pl.DeviceIdType.MESH
LANES = 128


class Phases:
    def __init__(self):
        self.open = None

    def __call__(self, name):
        if self.open is not None:
            self.open.__exit__(None, None, None)
        self.open = None
        if name is not None:
            self.open = jax.named_scope(name)
            self.open.__enter__()


def fused_kernel(
    sp_n, tp_n, score_scale,
    latent, condition_in, context, vector_in, modulator, gain_in,
    query_weight, key_weight, value_weight, head_gain_in, lambdas_in, bias_in, out_weight,
    out,
    condition, context_vector, norm_gain, head_gain, lambdas, context_bias,
    mod_v, part, rs_in, mods, lat, ctx_all, w_q, w_kv, w_out, vecs, hid, kvb, att_out, att_in,
    small_sem, own_sem, rs_ss, rs_rs, ag_ss, ag_rs, lat_ss, lat_rs, ctx_ss, ctx_rs,
    kv_os, kv_ss, kv_rs, wt_ss, wt_rs, wd_ss, wd_rs, at_ss, at_rs,
):
    sp = lax.axis_index("sp")
    tp = lax.axis_index("tp")
    dp = lax.axis_index("dp")
    n = sp_n * tp_n
    rank = sp * tp_n + tp
    half = lat.shape[1]
    width = lat.shape[2]
    rows = half * 2
    qrows = rows * tp_n
    chunk = part.shape[2]

    phase = Phases()
    phase("enter")
    barrier = pltpu.get_barrier_semaphore()

    def greet(d, carry):
        peer = lax.rem(rank + d, n)
        pl.semaphore_signal(
            barrier, inc=1, device_id=(peer // tp_n, lax.rem(peer, tp_n), dp), device_id_type=MESH
        )
        return carry

    lax.fori_loop(1, n, greet, 0)
    pl.semaphore_signal(barrier, inc=1, device_id=(sp, tp, 1 - dp), device_id_type=MESH)

    small = [
        pltpu.make_async_copy(source, place, small_sem.at[k])
        for k, (source, place) in enumerate((
            (condition_in, condition), (vector_in, context_vector), (context, ctx_all.at[sp]),
            (gain_in, norm_gain), (head_gain_in, head_gain), (lambdas_in, lambdas),
            (bias_in, context_bias),
        ))
    ]
    loads = [
        pltpu.make_async_copy(modulator, mod_v, own_sem.at[0]),
        pltpu.make_async_copy(latent, lat.at[pl.ds(tp * 2, 2)], own_sem.at[1]),
        pltpu.make_async_copy(key_weight, w_kv.at[:, pl.ds(0, LANES)], own_sem.at[2]),
        pltpu.make_async_copy(value_weight, w_kv.at[:, pl.ds(LANES, LANES)], own_sem.at[3]),
        pltpu.make_async_copy(query_weight, w_q, own_sem.at[4]),
        pltpu.make_async_copy(out_weight, w_out.at[pl.ds(tp * 4, 4)], own_sem.at[5]),
    ]
    for load in small[:2] + loads[:2] + small[2:] + loads[2:]:
        load.start()

    phase("partial")
    for load in small:
        load.wait()
    rows_in = jnp.concatenate([condition[...], context_vector[...]], axis=0).astype(jnp.float32)
    activated = jax.nn.silu(rows_in).astype(jnp.bfloat16)
    loads[0].wait()
    partial_terms = jnp.dot(activated, mod_v[...], preferred_element_type=jnp.float32)
    for p in range(n):
        part[p] = partial_terms[:, p * chunk : (p + 1) * chunk]
    loads[1].wait()
    phase("barrier")
    pl.semaphore_wait(barrier, n)
    phase("sends")

    def rs_copy(d):
        peer = lax.rem(rank + d, n)
        return pltpu.make_async_remote_copy(
            src_ref=part.at[peer], dst_ref=rs_in.at[d], send_sem=rs_ss.at[d], recv_sem=rs_rs.at[d],
            device_id=(peer // tp_n, lax.rem(peer, tp_n), dp), device_id_type=MESH,
        )

    def ag_copy(d):
        peer = lax.rem(rank + d, n)
        return pltpu.make_async_remote_copy(
            src_ref=mods.at[rank], dst_ref=mods.at[rank], send_sem=ag_ss.at[d], recv_sem=ag_rs.at[d],
            device_id=(peer // tp_n, lax.rem(peer, tp_n), dp), device_id_type=MESH,
        )

    def ag_arrival(d):
        peer = lax.rem(rank - d + n, n)
        return pltpu.make_async_remote_copy(
            src_ref=mods.at[peer], dst_ref=mods.at[peer], send_sem=ag_ss.at[d], recv_sem=ag_rs.at[d],
            device_id=(peer // tp_n, lax.rem(peer, tp_n), dp), device_id_type=MESH,
        )

    def each(first, last, act):
        def step(d, carry):
            act(d)
            return carry

        lax.fori_loop(first, last, step, 0)

    each(1, n, lambda d: rs_copy(d).start())

    across = tp + 1 - 2 * lax.rem(tp, 2)
    along = lax.rem(tp + 2, 4)
    corner = along + 1 - 2 * lax.rem(along, 2)

    class Plane:
        def __init__(self, buf, index, ss, rs):
            self.buf, self.index, self.ss, self.rs = buf, index, ss, rs

        def copy(self, owner, part_no, target, slot, kind):
            place = self.buf.at[self.index(owner, part_no)]
            return pltpu.make_async_remote_copy(
                src_ref=place, dst_ref=place, send_sem=self.ss.at[slot],
                recv_sem=self.rs.at[kind * 2 + part_no],
                device_id=(sp, target, dp), device_id_type=MESH,
            )

        def first(self):
            return [
                self.copy(tp, 0, across, 0, 0),
                self.copy(tp, 1, along, 1, 1),
                self.copy(tp, 1, across, 2, 0),
                self.copy(tp, 0, along, 3, 1),
            ]

        def relays(self):
            return [self.copy(across, 0, along, 4, 2), self.copy(along, 1, across, 5, 2)]

        def arrival(self, kind, part_no):
            owner = (across, along, corner)[kind]
            return self.copy(owner, part_no, across, 0, kind)

    plane = Plane(lat, lambda o, q: o * 2 + q, lat_ss, lat_rs)
    lat_first = plane.first()
    for copy in lat_first:
        copy.start()

    def ctx_copy(d):
        peer = lax.rem(sp + d, sp_n)
        return pltpu.make_async_remote_copy(
            src_ref=ctx_all.at[sp], dst_ref=ctx_all.at[sp], send_sem=ctx_ss.at[d], recv_sem=ctx_rs.at[d],
            device_id=(peer, tp, dp), device_id_type=MESH,
        )

    def ctx_arrival(d):
        peer = lax.rem(sp - d + sp_n, sp_n)
        return pltpu.make_async_remote_copy(
            src_ref=ctx_all.at[peer], dst_ref=ctx_all.at[peer], send_sem=ctx_ss.at[d], recv_sem=ctx_rs.at[d],
            device_id=(peer, tp, dp), device_id_type=MESH,
        )

    for d in range(1, sp_n):
        ctx_copy(d).start()
    rs_in[0] = part[rank]

    phase("rs_wait")
    each(1, n, lambda d: rs_copy(d).wait_recv())
    total = rs_in[0]
    for d in range(1, n):
        total = total + rs_in[d]
    mods[rank] = total
    each(1, n, lambda d: ag_copy(d).start())

    phase("lat_relay")
    lat_relays = plane.relays()
    plane.arrival(0, 0).wait_recv()
    lat_relays[0].start()
    plane.arrival(1, 1).wait_recv()
    lat_relays[1].start()

    loads[5].wait()
    wplane = Plane(w_out, lambda o, q: o * 4 + dp * 2 + q, wt_ss, wt_rs)
    w_first = wplane.first()
    for copy in w_first:
        copy.start()

    for d in range(1, sp_n):
        ctx_arrival(d).wait_recv()
    phase("ag_wait")
    each(1, n, lambda d: ag_arrival(d).wait_recv())
    whole = jnp.concatenate([mods[p] for p in range(n)], axis=1)
    phase("vecs")
    gain = norm_gain[...]
    vecs[0:1, :] = gain * (1.0 + whole[0:1, width : 2 * width])
    vecs[1:2, :] = whole[0:1, :width]
    vecs[2:3, :] = gain * (1.0 + whole[1:2, width : 2 * width])
    vecs[3:4, :] = whole[1:2, :width]
    vecs[4:5, :] = whole[0:1, 2 * width :]

    def normed_rows(x, at):
        x = x.astype(jnp.float32)
        scale = lax.rsqrt(jnp.mean(x * x, axis=-1, keepdims=True) + EPSILON)
        return (x * scale * vecs[at : at + 1, :] + vecs[at + 1 : at + 2, :]).astype(jnp.bfloat16)

    def norm_block(owner):
        for q in range(2):
            at = pl.multiple_of((owner * 2 + q) * half, half)
            hid[pl.ds(at, half), :] = normed_rows(lat[owner * 2 + q], 0)

    ctx_rows = ctx_all.shape[0] * ctx_all.shape[1]
    hid[qrows : qrows + ctx_rows, :] = normed_rows(
        ctx_all[...].astype(jnp.float32).reshape(ctx_rows, width), 2
    )
    norm_block(tp)
    phase("lat_rest")
    plane.arrival(0, 1).wait_recv()
    norm_block(across)
    plane.arrival(1, 0).wait_recv()
    norm_block(along)
    plane.arrival(2, 0).wait_recv()
    plane.arrival(2, 1).wait_recv()
    norm_block(corner)

    phase("kv")
    for load in loads[2:5]:
        load.wait()
    kv = jnp.dot(hid[...], w_kv[...], preferred_element_type=jnp.float32).astype(jnp.bfloat16)
    piece = qrows // 2
    for q in range(2):
        kvb[sp * 2 + q] = kv[q * piece : (q + 1) * piece]
    ctx_kv = kv[qrows:]

    def kv_own(to, slot, q):
        place = kvb.at[sp * 2 + q]
        return pltpu.make_async_remote_copy(
            src_ref=place, dst_ref=place, send_sem=kv_os.at[slot * 2 + q],
            recv_sem=kv_rs.at[sp * 2 + q], device_id=(to, tp, dp), device_id_type=MESH,
        )

    for q in range(2):
        pl.when(sp + 1 < sp_n)(lambda: kv_own(sp + 1, 0, q).start())
        pl.when(sp > 0)(lambda: kv_own(sp - 1, 1, q).start())

    phase("queries")
    queries = jnp.dot(hid[:qrows, :], w_q[...], preferred_element_type=jnp.float32) * score_scale
    queries = queries.astype(jnp.bfloat16)
    head = queries.shape[1] // 2
    lane = lax.broadcasted_iota(jnp.int32, queries.shape, 1)
    zero = jnp.zeros_like(queries)
    both = jnp.concatenate(
        [jnp.where(lane < head, queries, zero), jnp.where(lane < head, zero, queries)], axis=0
    )

    def score(keys):
        return lax.dot_general(
            both, keys, (((1,), (1,)), ((), ())), preferred_element_type=jnp.float32
        )

    map_row = lax.broadcasted_iota(jnp.int32, (2 * qrows, 1), 0)
    bias = jnp.where(map_row < qrows, context_bias[0:1, 0:1], context_bias[0:1, 1:2])

    def fold(running, scores, values):
        top = jnp.max(scores, axis=-1, keepdims=True)
        if running is not None:
            top = jnp.maximum(running[0], top)
        weights = jnp.exp(scores - top)
        count = jnp.sum(weights, axis=-1, keepdims=True)
        summed = jnp.dot(weights.astype(jnp.bfloat16), values, preferred_element_type=jnp.float32)
        if running is not None:
            shrink = jnp.exp(running[0] - top)
            count = running[1] * shrink + count
            summed = running[2] * shrink + summed
        return top, count, summed

    phase("fold_own")
    running = fold(None, score(ctx_kv[:, :LANES]) + bias, ctx_kv[:, LANES:])
    running = fold(running, score(kv[:qrows, :LANES]), kv[:qrows, LANES:])

    def sibling(owner, part_no, slot):
        place = w_out.at[owner * 4 + dp * 2 + part_no]
        return pltpu.make_async_remote_copy(
            src_ref=place, dst_ref=place, send_sem=wd_ss.at[slot], recv_sem=wd_rs.at[slot],
            device_id=(sp, tp, 1 - dp), device_id_type=MESH,
        )

    def sibling_arrival(owner, part_no, slot):
        place = w_out.at[owner * 4 + (1 - dp) * 2 + part_no]
        return pltpu.make_async_remote_copy(
            src_ref=place, dst_ref=place, send_sem=wd_ss.at[slot], recv_sem=wd_rs.at[slot],
            device_id=(sp, tp, 1 - dp), device_id_type=MESH,
        )

    owners = (across, along, corner)
    w_sent = []

    def swap(kind, part_no, wait=True):
        if wait:
            wplane.arrival(kind, part_no).wait_recv()
        copy = sibling(owners[kind], part_no, kind * 2 + part_no)
        copy.start()
        w_sent.append(copy)

    phase("w_relay")
    w_relays = wplane.relays()
    wplane.arrival(0, 0).wait_recv()
    w_relays[0].start()
    wplane.arrival(1, 1).wait_recv()
    w_relays[1].start()
    swap(0, 0, False)
    swap(1, 1, False)

    high = (2 * sp) // sp_n

    def block_at(t):
        up = (t - 1) + jnp.where(t - 1 >= sp, 1, 0)
        down = (sp_n - t) - jnp.where(sp_n - t <= sp, 1, 0)
        return jnp.where(high == 0, up, down)

    def onward(b, q):
        step = jnp.where(b < sp, 1, -1)
        to = sp + step
        ok = jnp.logical_and(to >= 0, to < sp_n)
        safe = jnp.where(ok, to, sp - step)
        return ok, pltpu.make_async_remote_copy(
            src_ref=kvb.at[b * 2 + q], dst_ref=kvb.at[b * 2 + q], send_sem=kv_ss.at[b * 2 + q],
            recv_sem=kv_rs.at[b * 2 + q], device_id=(safe, tp, dp), device_id_type=MESH,
        )

    sent = []
    for pair in range(1, sp_n, 2):
        steps = [t for t in (pair, pair + 1) if t < sp_n]
        phase(f"take{pair}")
        for q in range(2):
            for t in steps:
                ok, copy = onward(block_at(t), q)
                copy.wait_recv()
                pl.when(ok)(copy.start)
                sent.append((ok, copy))
        phase(f"fold{pair}")
        if pair == 1:
            swap(0, 1)
            swap(1, 0)
        for t in steps:
            block = kvb[pl.ds(block_at(t) * 2, 2)].reshape(qrows, 2 * LANES)
            running = fold(running, score(block[:, :LANES]), block[:, LANES:])

    phase("finish")
    top, count, summed = running
    shares = summed / count
    mixed = shares[:qrows] - lambdas[...] * shares[qrows:]
    normed = (
        mixed
        * lax.rsqrt(jnp.mean(mixed * mixed, axis=-1, keepdims=True) + EPSILON)
        * head_gain[...]
        * OUT_SCALE
    ).astype(jnp.bfloat16)
    for p in range(tp_n):
        att_out[p] = normed[p * rows : (p + 1) * rows]

    def at_copy(d):
        peer = lax.rem(tp + d, tp_n)
        return pltpu.make_async_remote_copy(
            src_ref=att_out.at[peer], dst_ref=att_in.at[tp], send_sem=at_ss.at[d], recv_sem=at_rs.at[d],
            device_id=(sp, peer, dp), device_id_type=MESH,
        )

    def at_arrival(d):
        peer = lax.rem(tp - d + tp_n, tp_n)
        return pltpu.make_async_remote_copy(
            src_ref=att_out.at[peer], dst_ref=att_in.at[peer], send_sem=at_ss.at[d], recv_sem=at_rs.at[d],
            device_id=(sp, peer, dp), device_id_type=MESH,
        )

    for d in range(1, tp_n):
        at_copy(d).start()
    att_in[tp] = att_out[tp]

    phase("w_wait")
    swap(2, 0)
    swap(2, 1)
    for kind in range(3):
        for part_no in range(2):
            sibling_arrival(owners[kind], part_no, kind * 2 + part_no).wait_recv()
    phase("at_wait")
    for d in range(1, tp_n):
        at_arrival(d).wait_recv()

    phase("out")
    attended = jnp.concatenate([att_in[p] for p in range(tp_n)], axis=1)
    step = 512
    for first in range(0, width, step):
        cols = slice(first, first + step)
        weight = w_out[:, :, cols].reshape(attended.shape[1], step)
        branch = jnp.dot(attended, weight, preferred_element_type=jnp.float32)
        for q in range(2):
            mine = lat[tp * 2 + q, :, cols].astype(jnp.float32)
            update = mine + vecs[4:5, cols] * branch[q * half : (q + 1) * half]
            out[q * half : (q + 1) * half, cols] = update.astype(jnp.bfloat16)

    phase("drain")
    each(1, n, lambda d: rs_copy(d).wait_send())
    each(1, n, lambda d: ag_copy(d).wait_send())
    for copy in lat_first + lat_relays + w_first + w_relays + w_sent:
        copy.wait_send()
    for d in range(1, sp_n):
        ctx_copy(d).wait_send()
    for q in range(2):
        pl.when(sp + 1 < sp_n)(lambda: kv_own(sp + 1, 0, q).wait_send())
        pl.when(sp > 0)(lambda: kv_own(sp - 1, 1, q).wait_send())
    for ok, copy in sent:
        pl.when(ok)(copy.wait_send)
    for d in range(1, tp_n):
        at_copy(d).wait_send()
    phase(None)


def fused(
    axes, latent, condition, context, context_vector, modulator, norm_gain, query_weight,
    key_weight, value_weight, head_gain, lambdas, context_bias, out_weight,
):
    sp_n, tp_n, dp_n = axes
    n = sp_n * tp_n
    rows, width = latent.shape[1:]
    half = rows // 2
    chunk = modulator.shape[1] // n
    ctx_rows = context.shape[1]
    qw = query_weight.shape[1]
    value = value_weight.shape[1]
    qrows = rows * tp_n
    wrows = out_weight.shape[0] // 4
    bf, f32 = jnp.bfloat16, jnp.float32
    vm = pl.BlockSpec(memory_space=pltpu.VMEM)
    hb = pl.BlockSpec(memory_space=pltpu.HBM)
    dma = lambda k: pltpu.SemaphoreType.DMA((k,))
    result = pl.pallas_call(
        functools.partial(fused_kernel, sp_n, tp_n, (qw // 2) ** (-0.5)),
        out_shape=pltpu.VMEM((rows, width), bf),
        in_specs=[hb] * 13,
        out_specs=vm,
        scratch_shapes=[
            pltpu.VMEM(condition.shape, bf),
            pltpu.VMEM((1, context_vector.shape[0]), bf),
            pltpu.VMEM((1, width), f32),
            pltpu.VMEM((1, value), f32),
            pltpu.VMEM((1, 1), f32),
            pltpu.VMEM(context_bias.shape, f32),
            pltpu.VMEM(modulator.shape, bf),
            pltpu.VMEM((n, 2, chunk), f32),
            pltpu.VMEM((n, 2, chunk), f32),
            pltpu.VMEM((n, 2, chunk), f32),
            pltpu.VMEM((tp_n * 2, half, width), bf),
            pltpu.VMEM((sp_n, ctx_rows, width), bf),
            pltpu.VMEM((width, qw), bf),
            pltpu.VMEM((width, qw + value), bf),
            pltpu.VMEM((tp_n * 4, wrows, width), bf),
            pltpu.VMEM((8, width), f32),
            pltpu.VMEM((qrows + sp_n * ctx_rows, width), bf),
            pltpu.VMEM((sp_n * 2, qrows // 2, qw + value), bf),
            pltpu.VMEM((tp_n, rows, value), bf),
            pltpu.VMEM((tp_n, rows, value), bf),
            dma(7), dma(6), dma(n), dma(n), dma(n), dma(n), dma(6), dma(6), dma(sp_n), dma(sp_n),
            dma(4), dma(sp_n * 2), dma(sp_n * 2), dma(6), dma(6), dma(6), dma(6), dma(tp_n), dma(tp_n),
        ],
        compiler_params=pltpu.CompilerParams(
            collective_id=0, has_side_effects=True, vmem_limit_bytes=66700000
        ),
        name="fused_block",
    )(
        latent.reshape(2, half, width),
        condition,
        context[0],
        context_vector[None, :],
        modulator,
        norm_gain[None, :],
        query_weight,
        key_weight,
        value_weight,
        head_gain[None, :],
        lambdas[None, :],
        context_bias,
        out_weight.reshape(4, wrows, width),
    )
    return result[None]


def choose(axes, *arrays):
    sp_n, tp_n, dp_n = axes
    latent, modulator, query_weight, value_weight = arrays[0], arrays[4], arrays[6], arrays[8]
    lambdas, out_weight = arrays[10], arrays[12]
    fits = (
        tp_n == 4
        and dp_n == 2
        and 1 < sp_n <= 8
        and lambdas.shape[0] == 1
        and query_weight.shape[1] == LANES
        and value_weight.shape[1] == LANES
        and modulator.shape[1] % (sp_n * tp_n * LANES) == 0
        and latent.shape[1] % 32 == 0
        and latent.shape[2] % 512 == 0
        and out_weight.shape[0] % 64 == 0
    )
    return fused(axes, *arrays) if fits else body(*arrays)


def solution(mesh):
    placed = (
        P("dp", ("sp", "tp"), None),
        P("dp", ("sp", "tp")),
        P("dp", "sp", None),
        P(("sp", "tp")),
        P(("sp", "tp"), None),
        P(),
        P(None, "tp"),
        P(None, "tp"),
        P(None, "tp"),
        P(),
        P("tp"),
        P("tp", None),
        P("tp", None),
    )
    axes = (mesh.shape["sp"], mesh.shape["tp"], mesh.shape["dp"])
    return jax.shard_map(
        functools.partial(choose, axes), mesh=mesh, in_specs=placed, out_specs=P("dp", ("sp", "tp"), None), check_vma=False
    )
```

```python
import functools

import jax
import jax.numpy as jnp
from jax import lax
from jax.experimental import pallas as pl
from jax.experimental.pallas import tpu as pltpu
from jax.sharding import PartitionSpec as P

EPSILON = 1e-06
OUT_SCALE = 0.8
KEY_BLOCK = 2048
LOW_START = -1e30


def modulate(inputs, gain_vector, shift_vector, scale_vector):
    as_float = inputs.astype(jnp.float32)
    normed = as_float * lax.rsqrt(jnp.mean(as_float * as_float, axis=-1, keepdims=True) + EPSILON)
    return (normed * gain_vector * (1.0 + scale_vector) + shift_vector).astype(jnp.bfloat16)


def fold_block(running, queries, keys_in, values_in, key_flags, bias_table, score_scale):
    run_max, run_total, summed = running
    scores = (
        jnp.einsum("qhmd,khmd->hmqk", queries, keys_in, preferred_element_type=jnp.float32)
        * score_scale
    )
    if key_flags is not None:
        scores = scores + bias_table[:, :, None, None] * key_flags
    new_max = jnp.maximum(run_max, jnp.max(scores, axis=-1))
    shrink = jnp.exp(run_max - new_max)
    weights = jnp.exp(scores - new_max[..., None])
    run_total = run_total * shrink + jnp.sum(weights, axis=-1)
    summed = summed * shrink[..., None] + jnp.einsum(
        "hmqk,khe->hmqe",
        weights.astype(jnp.bfloat16),
        values_in,
        preferred_element_type=jnp.float32,
    )
    return (new_max, run_total, summed)


def fold_keys(running, queries, keys_in, values_in, key_flags, bias_table, score_scale):
    full_blocks = keys_in.shape[0] // KEY_BLOCK
    if full_blocks > 1:
        edge = full_blocks * KEY_BLOCK
        stacked = (
            keys_in[:edge].reshape((full_blocks, KEY_BLOCK) + keys_in.shape[1:]),
            values_in[:edge].reshape((full_blocks, KEY_BLOCK) + values_in.shape[1:]),
        )
        if key_flags is not None:
            stacked = stacked + (key_flags[:edge].reshape(full_blocks, KEY_BLOCK),)

        def fold_step(current, block_data):
            flag_part = None if key_flags is None else block_data[2]
            return (
                fold_block(
                    current,
                    queries,
                    block_data[0],
                    block_data[1],
                    flag_part,
                    bias_table,
                    score_scale,
                ),
                None,
            )

        running, ignored = lax.scan(fold_step, running, stacked)
        keys_in = keys_in[edge:]
        values_in = values_in[edge:]
        key_flags = None if key_flags is None else key_flags[edge:]
    if keys_in.shape[0] > 0:
        running = fold_block(
            running, queries, keys_in, values_in, key_flags, bias_table, score_scale
        )
    return running


def body(
    latent,
    condition,
    context,
    context_vector,
    modulator,
    norm_gain,
    query_weight,
    key_weight,
    value_weight,
    head_gain,
    lambdas,
    context_bias,
    out_weight,
):
    model_width = latent.shape[2]
    local_heads = lambdas.shape[0]
    query_width = query_weight.shape[1]
    head_size = query_width // (2 * local_heads)
    value_size = value_weight.shape[1] // local_heads
    score_scale = head_size ** (-0.5)
    activated = jax.nn.silu(
        jnp.concatenate([condition, context_vector[None, :]], axis=0).astype(jnp.float32)
    )
    partial_terms = jnp.dot(
        activated.astype(jnp.bfloat16), modulator, preferred_element_type=jnp.float32
    )
    modulations = lax.psum(partial_terms, ("sp", "tp"))
    hidden = modulate(
        latent[0],
        norm_gain,
        modulations[0, :model_width],
        modulations[0, model_width : 2 * model_width],
    )
    ctx_hidden = modulate(
        context[0],
        norm_gain,
        modulations[1, :model_width],
        modulations[1, model_width : 2 * model_width],
    )
    gate_vector = modulations[0, 2 * model_width :]
    incoming = lax.all_gather(hidden, "tp", axis=0, tiled=True)
    projected = jnp.concatenate(
        [
            jnp.dot(incoming, query_weight, preferred_element_type=jnp.float32),
            jnp.dot(incoming, key_weight, preferred_element_type=jnp.float32),
            jnp.dot(incoming, value_weight, preferred_element_type=jnp.float32),
        ],
        axis=1,
    ).astype(jnp.bfloat16)
    query_rows = projected.shape[0]
    queries = projected[:, :query_width].reshape(query_rows, local_heads, 2, head_size)
    own_keys = projected[:, query_width : 2 * query_width]
    own_values = projected[:, 2 * query_width :]
    gathered_context = lax.all_gather(ctx_hidden, "sp", axis=0, tiled=True)
    ctx_keys = jnp.dot(gathered_context, key_weight, preferred_element_type=jnp.float32).astype(
        jnp.bfloat16
    )
    ctx_values = jnp.dot(gathered_context, value_weight, preferred_element_type=jnp.float32).astype(
        jnp.bfloat16
    )
    start_carry = (
        jnp.full((local_heads, 2, query_rows), LOW_START, jnp.float32),
        jnp.zeros((local_heads, 2, query_rows), jnp.float32),
        jnp.zeros((local_heads, 2, query_rows, value_size), jnp.float32),
    )
    pieces = (own_keys, own_values)
    initial = fold_keys(
        start_carry,
        queries,
        ctx_keys.reshape(-1, local_heads, 2, head_size),
        ctx_values.reshape(-1, local_heads, value_size),
        jnp.ones((ctx_keys.shape[0],), jnp.float32),
        context_bias,
        score_scale,
    )
    incoming = (
        lax.all_gather(pieces[0], "sp", axis=0, tiled=True),
        lax.all_gather(pieces[1], "sp", axis=0, tiled=True),
    )
    run_max, run_total, summed = fold_keys(
        initial,
        queries,
        incoming[0].reshape(-1, local_heads, 2, head_size),
        incoming[1].reshape(-1, local_heads, value_size),
        None,
        context_bias,
        score_scale,
    )
    mixed = (
        summed[:, 0] / run_total[:, 0, :, None]
        - lambdas[:, None, None] * summed[:, 1] / run_total[:, 1, :, None]
    )
    normed = (
        mixed
        * lax.rsqrt(jnp.mean(mixed * mixed, axis=-1, keepdims=True) + EPSILON)
        * head_gain
        * OUT_SCALE
    )
    attended = (
        jnp.transpose(normed, (1, 0, 2))
        .reshape(query_rows, local_heads * value_size)
        .astype(jnp.bfloat16)
    )
    exchanged = lax.all_to_all(attended, "tp", split_axis=0, concat_axis=1, tiled=True)
    whole_weight = lax.all_gather(out_weight, "tp", axis=0, tiled=True)
    branch = jnp.dot(exchanged, whole_weight, preferred_element_type=jnp.float32)
    result = (latent[0].astype(jnp.float32) + gate_vector * branch).astype(jnp.bfloat16)
    return result[None]


MESH = pl.DeviceIdType.MESH
LANES = 128


class Phases:
    def __init__(self):
        self.open = None

    def __call__(self, name):
        if self.open is not None:
            self.open.__exit__(None, None, None)
        self.open = None
        if name is not None:
            self.open = jax.named_scope(name)
            self.open.__enter__()


def fused_kernel(
    sp_n, tp_n, score_scale,
    latent, condition_in, context, vector_in, modulator, gain_in,
    query_weight, key_weight, value_weight, head_gain_in, lambdas_in, bias_in, out_weight,
    out,
    condition, context_vector, norm_gain, head_gain, lambdas, context_bias,
    mod_v, part, rs_in, mods, lat, ctx_all, w_q, w_kv, w_out, vecs, hid, kvb, att_out, att_in,
    small_sem, own_sem, rs_ss, rs_rs, ag_ss, ag_rs, lat_ss, lat_rs, ctx_ss, ctx_rs,
    kv_os, kv_ss, kv_rs, wt_ss, wt_rs, wd_ss, wd_rs, at_ss, at_rs,
):
    sp = lax.axis_index("sp")
    tp = lax.axis_index("tp")
    dp = lax.axis_index("dp")
    n = sp_n * tp_n
    rank = sp * tp_n + tp
    across = tp + 1 - 2 * lax.rem(tp, 2)
    along = lax.rem(tp + 2, 4)
    corner = along + 1 - 2 * lax.rem(along, 2)
    roles = (tp, across, along, corner)
    half = lat.shape[1]
    width = lat.shape[2]
    rows = half * 2
    qrows = rows * tp_n
    chunk = part.shape[2]

    phase = Phases()
    phase("enter")
    barrier = pltpu.get_barrier_semaphore()

    small = [
        pltpu.make_async_copy(source, place, small_sem.at[k])
        for k, (source, place) in enumerate((
            (condition_in, condition), (vector_in, context_vector), (context, ctx_all.at[sp]),
            (gain_in, norm_gain), (head_gain_in, head_gain), (lambdas_in, lambdas),
            (bias_in, context_bias),
        ))
    ]
    loads = [
        pltpu.make_async_copy(modulator, mod_v, own_sem.at[0]),
        pltpu.make_async_copy(latent, lat.at[pl.ds(tp * 2, 2)], own_sem.at[1]),
        pltpu.make_async_copy(key_weight, w_kv.at[:, pl.ds(0, LANES)], own_sem.at[2]),
        pltpu.make_async_copy(value_weight, w_kv.at[:, pl.ds(LANES, LANES)], own_sem.at[3]),
        pltpu.make_async_copy(query_weight, w_q, own_sem.at[4]),
        pltpu.make_async_copy(out_weight, w_out.at[pl.ds(tp * 4, 4)], own_sem.at[5]),
    ]
    for load in small[:2] + loads[:2] + small[2:] + loads[2:]:
        load.start()

    def greet(d, carry):
        peer = lax.rem(rank + d, n)
        pl.semaphore_signal(
            barrier, inc=1, device_id=(peer // tp_n, lax.rem(peer, tp_n), dp), device_id_type=MESH
        )
        return carry

    lax.fori_loop(1, n, greet, 0)
    pl.semaphore_signal(barrier, inc=1, device_id=(sp, tp, 1 - dp), device_id_type=MESH)

    phase("partial")
    for load in small:
        load.wait()
    rows_in = jnp.concatenate([condition[...], context_vector[...]], axis=0).astype(jnp.float32)
    activated = jax.nn.silu(rows_in).astype(jnp.bfloat16)
    loads[0].wait()
    partial_terms = jnp.dot(activated, mod_v[...], preferred_element_type=jnp.float32)
    for p in range(n):
        part[p] = partial_terms[:, p * chunk : (p + 1) * chunk]
    loads[1].wait()
    phase("barrier")
    pl.semaphore_wait(barrier, n)
    phase("sends")

    def rs_copy(d):
        peer = lax.rem(rank + d, n)
        return pltpu.make_async_remote_copy(
            src_ref=part.at[peer], dst_ref=rs_in.at[d], send_sem=rs_ss.at[0], recv_sem=rs_rs.at[0],
            device_id=(peer // tp_n, lax.rem(peer, tp_n), dp), device_id_type=MESH,
        )

    def ag_copy(d):
        peer = lax.rem(rank + d, n)
        return pltpu.make_async_remote_copy(
            src_ref=mods.at[rank], dst_ref=mods.at[rank], send_sem=ag_ss.at[0], recv_sem=ag_rs.at[0],
            device_id=(peer // tp_n, lax.rem(peer, tp_n), dp), device_id_type=MESH,
        )

    def rs_all():
        return pltpu.make_async_remote_copy(
            src_ref=part.at[pl.ds(0, n - 1)], dst_ref=rs_in.at[pl.ds(1, n - 1)],
            send_sem=rs_ss.at[0], recv_sem=rs_rs.at[0],
            device_id=(sp, across, dp), device_id_type=MESH,
        )

    def ag_all():
        return pltpu.make_async_remote_copy(
            src_ref=mods.at[pl.ds(0, n - 1)], dst_ref=mods.at[pl.ds(0, n - 1)],
            send_sem=ag_ss.at[0], recv_sem=ag_rs.at[0],
            device_id=(sp, across, dp), device_id_type=MESH,
        )

    def each(first, last, act):
        def step(d, carry):
            act(d)
            return carry

        lax.fori_loop(first, last, step, 0)

    each(1, n, lambda d: rs_copy(d).start())


    class Plane:
        def __init__(self, buf, index, ss, rs):
            self.buf, self.index, self.ss, self.rs = buf, index, ss, rs

        def copy(self, owner, part_no, target, slot, kind):
            place = self.buf.at[self.index(owner, part_no)]
            return pltpu.make_async_remote_copy(
                src_ref=place, dst_ref=place, send_sem=self.ss.at[slot],
                recv_sem=self.rs.at[kind * 2 + part_no],
                device_id=(sp, target, dp), device_id_type=MESH,
            )

        def first(self):
            return [
                self.copy(tp, 0, across, 0, 0),
                self.copy(tp, 1, along, 1, 1),
                self.copy(tp, 1, across, 2, 0),
                self.copy(tp, 0, along, 3, 1),
            ]

        def relays(self):
            return [self.copy(across, 0, along, 4, 2), self.copy(along, 1, across, 5, 2)]

        def arrival(self, kind, part_no):
            owner = (across, along, corner)[kind]
            return self.copy(owner, part_no, across, 0, kind)

    plane = Plane(lat, lambda o, q: o * 2 + q, lat_ss, lat_rs)
    lat_first = plane.first()
    for copy in lat_first:
        copy.start()

    def ctx_copy(d):
        peer = lax.rem(sp + d, sp_n)
        return pltpu.make_async_remote_copy(
            src_ref=ctx_all.at[sp], dst_ref=ctx_all.at[sp], send_sem=ctx_ss.at[d], recv_sem=ctx_rs.at[d],
            device_id=(peer, tp, dp), device_id_type=MESH,
        )

    def ctx_arrival(d):
        peer = lax.rem(sp - d + sp_n, sp_n)
        return pltpu.make_async_remote_copy(
            src_ref=ctx_all.at[peer], dst_ref=ctx_all.at[peer], send_sem=ctx_ss.at[d], recv_sem=ctx_rs.at[d],
            device_id=(peer, tp, dp), device_id_type=MESH,
        )

    for d in range(1, sp_n):
        ctx_copy(d).start()
    rs_in[0] = part[rank]

    phase("rs_wait")
    rs_all().wait_recv()
    total = rs_in[0]
    for d in range(1, n):
        total = total + rs_in[d]
    mods[rank] = total
    each(1, n, lambda d: ag_copy(d).start())

    phase("lat_relay")
    lat_relays = plane.relays()
    plane.arrival(0, 0).wait_recv()
    lat_relays[0].start()
    plane.arrival(1, 1).wait_recv()
    lat_relays[1].start()

    loads[5].wait()
    wplane = Plane(w_out, lambda o, q: o * 4 + dp * 2 + q, wt_ss, wt_rs)
    w_first = wplane.first()
    for copy in w_first:
        copy.start()

    for d in range(1, sp_n):
        ctx_arrival(d).wait_recv()
    phase("ag_wait")
    ag_all().wait_recv()
    whole = jnp.concatenate([mods[p] for p in range(n)], axis=1)
    phase("vecs")
    gain = norm_gain[...]
    vecs[0:1, :] = gain * (1.0 + whole[0:1, width : 2 * width])
    vecs[1:2, :] = whole[0:1, :width]
    vecs[2:3, :] = gain * (1.0 + whole[1:2, width : 2 * width])
    vecs[3:4, :] = whole[1:2, :width]
    vecs[4:5, :] = whole[0:1, 2 * width :]

    def normed_rows(x, at):
        x = x.astype(jnp.float32)
        scale = lax.rsqrt(jnp.mean(x * x, axis=-1, keepdims=True) + EPSILON)
        return (x * scale * vecs[at : at + 1, :] + vecs[at + 1 : at + 2, :]).astype(jnp.bfloat16)

    def norm_block(role):
        for q in range(2):
            at = (role * 2 + q) * half
            hid[at : at + half, :] = normed_rows(lat[roles[role] * 2 + q], 0)

    def kv_own(to, slot, q):
        place = kvb.at[sp * 2 + q]
        return pltpu.make_async_remote_copy(
            src_ref=place, dst_ref=place, send_sem=kv_os.at[slot * 2 + q],
            recv_sem=kv_rs.at[sp * 2 + q], device_id=(to, tp, dp), device_id_type=MESH,
        )

    def kv_rows(first, last):
        product = jnp.dot(hid[first:last, :], w_kv[...], preferred_element_type=jnp.float32)
        return product.astype(jnp.bfloat16)

    def kv_send(q):
        pl.when(sp + 1 < sp_n)(lambda: kv_own(sp + 1, 0, q).start())
        pl.when(sp > 0)(lambda: kv_own(sp - 1, 1, q).start())

    piece = qrows // 2
    ctx_rows = ctx_all.shape[0] * ctx_all.shape[1]
    norm_block(0)
    plane.arrival(0, 1).wait_recv()
    norm_block(1)
    phase("kv0")
    for load in loads[2:5]:
        load.wait()
    kv_near = kv_rows(0, piece)
    kvb[sp * 2] = kv_near
    kv_send(0)
    phase("lat_rest")
    hid[qrows : qrows + ctx_rows, :] = normed_rows(
        ctx_all[...].astype(jnp.float32).reshape(ctx_rows, width), 2
    )
    plane.arrival(1, 0).wait_recv()
    norm_block(2)
    plane.arrival(2, 0).wait_recv()
    plane.arrival(2, 1).wait_recv()
    norm_block(3)
    phase("kv1")
    kv_far = kv_rows(piece, qrows + ctx_rows)
    kvb[sp * 2 + 1] = kv_far[:piece]
    kv_send(1)
    kv = jnp.concatenate([kv_near, kv_far[:piece]], axis=0)
    ctx_kv = kv_far[piece:]

    phase("queries")
    queries = jnp.dot(hid[:qrows, :], w_q[...], preferred_element_type=jnp.float32) * score_scale
    queries = queries.astype(jnp.bfloat16)
    head = queries.shape[1] // 2
    lane = lax.broadcasted_iota(jnp.int32, queries.shape, 1)
    zero = jnp.zeros_like(queries)
    both = jnp.concatenate(
        [jnp.where(lane < head, queries, zero), jnp.where(lane < head, zero, queries)], axis=0
    )

    def score(keys):
        return lax.dot_general(
            both, keys, (((1,), (1,)), ((), ())), preferred_element_type=jnp.float32
        )

    map_row = lax.broadcasted_iota(jnp.int32, (2 * qrows, 1), 0)
    bias = jnp.where(map_row < qrows, context_bias[0:1, 0:1], context_bias[0:1, 1:2])

    def fold(running, scores, values):
        top = jnp.max(scores, axis=-1, keepdims=True)
        if running is not None:
            top = jnp.maximum(running[0], top)
        weights = jnp.exp(scores - top)
        count = jnp.sum(weights, axis=-1, keepdims=True)
        summed = jnp.dot(weights.astype(jnp.bfloat16), values, preferred_element_type=jnp.float32)
        if running is not None:
            shrink = jnp.exp(running[0] - top)
            count = running[1] * shrink + count
            summed = running[2] * shrink + summed
        return top, count, summed

    phase("fold_own")
    running = fold(None, score(ctx_kv[:, :LANES]) + bias, ctx_kv[:, LANES:])
    running = fold(running, score(kv[:, :LANES]), kv[:, LANES:])

    def sibling(owner, part_no, slot):
        place = w_out.at[owner * 4 + dp * 2 + part_no]
        return pltpu.make_async_remote_copy(
            src_ref=place, dst_ref=place, send_sem=wd_ss.at[slot], recv_sem=wd_rs.at[slot],
            device_id=(sp, tp, 1 - dp), device_id_type=MESH,
        )

    def sibling_arrival(owner, part_no, slot):
        place = w_out.at[owner * 4 + (1 - dp) * 2 + part_no]
        return pltpu.make_async_remote_copy(
            src_ref=place, dst_ref=place, send_sem=wd_ss.at[slot], recv_sem=wd_rs.at[slot],
            device_id=(sp, tp, 1 - dp), device_id_type=MESH,
        )

    owners = (across, along, corner)
    w_sent = []

    def swap(kind, part_no, wait=True):
        if wait:
            wplane.arrival(kind, part_no).wait_recv()
        copy = sibling(owners[kind], part_no, kind * 2 + part_no)
        copy.start()
        w_sent.append(copy)

    phase("w_relay")
    w_relays = wplane.relays()
    wplane.arrival(0, 0).wait_recv()
    w_relays[0].start()
    wplane.arrival(1, 1).wait_recv()
    w_relays[1].start()
    swap(0, 0, False)
    swap(1, 1, False)

    high = (2 * sp) // sp_n

    def block_at(t):
        up = (t - 1) + jnp.where(t - 1 >= sp, 1, 0)
        down = (sp_n - t) - jnp.where(sp_n - t <= sp, 1, 0)
        return jnp.where(high == 0, up, down)

    def onward(b, q):
        step = jnp.where(b < sp, 1, -1)
        to = sp + step
        ok = jnp.logical_and(to >= 0, to < sp_n)
        safe = jnp.where(ok, to, sp - step)
        return ok, pltpu.make_async_remote_copy(
            src_ref=kvb.at[b * 2 + q], dst_ref=kvb.at[b * 2 + q], send_sem=kv_ss.at[b * 2 + q],
            recv_sem=kv_rs.at[b * 2 + q], device_id=(safe, tp, dp), device_id_type=MESH,
        )

    sent = []
    for pair in range(1, sp_n, 2):
        steps = [t for t in (pair, pair + 1) if t < sp_n]
        phase(f"take{pair}")
        for q in range(2):
            for t in steps:
                ok, copy = onward(block_at(t), q)
                copy.wait_recv()
                pl.when(ok)(copy.start)
                sent.append((ok, copy))
        phase(f"fold{pair}")
        if pair == 1:
            swap(0, 1)
            swap(1, 0)
        for t in steps:
            block = kvb[pl.ds(block_at(t) * 2, 2)].reshape(qrows, 2 * LANES)
            running = fold(running, score(block[:, :LANES]), block[:, LANES:])

    phase("finish")
    top, count, summed = running
    shares = summed / count
    mixed = shares[:qrows] - lambdas[...] * shares[qrows:]
    normed = (
        mixed
        * lax.rsqrt(jnp.mean(mixed * mixed, axis=-1, keepdims=True) + EPSILON)
        * head_gain[...]
        * OUT_SCALE
    ).astype(jnp.bfloat16)
    for p in range(tp_n):
        att_out[p] = normed[p * rows : (p + 1) * rows]

    def at_copy(d):
        return pltpu.make_async_remote_copy(
            src_ref=att_out.at[d], dst_ref=att_in.at[tp], send_sem=at_ss.at[d], recv_sem=at_rs.at[d],
            device_id=(sp, roles[d], dp), device_id_type=MESH,
        )

    def at_arrival(d):
        return pltpu.make_async_remote_copy(
            src_ref=att_out.at[d], dst_ref=att_in.at[roles[d]], send_sem=at_ss.at[d],
            recv_sem=at_rs.at[d], device_id=(sp, roles[d], dp), device_id_type=MESH,
        )

    for d in (3, 1, 2):
        at_copy(d).start()
    att_in[tp] = att_out[0]

    phase("w_wait")
    swap(2, 0)
    swap(2, 1)
    for kind in range(3):
        for part_no in range(2):
            sibling_arrival(owners[kind], part_no, kind * 2 + part_no).wait_recv()
    phase("at_wait")
    for d in range(1, tp_n):
        at_arrival(d).wait_recv()

    phase("out")
    attended = jnp.concatenate([att_in[p] for p in range(tp_n)], axis=1)
    step = 512
    for first in range(0, width, step):
        cols = slice(first, first + step)
        weight = w_out[:, :, cols].reshape(attended.shape[1], step)
        branch = jnp.dot(attended, weight, preferred_element_type=jnp.float32)
        for q in range(2):
            mine = lat[tp * 2 + q, :, cols].astype(jnp.float32)
            update = mine + vecs[4:5, cols] * branch[q * half : (q + 1) * half]
            out[q * half : (q + 1) * half, cols] = update.astype(jnp.bfloat16)

    phase("drain")
    rs_all().wait_send()
    ag_all().wait_send()
    for copy in lat_first + lat_relays + w_first + w_relays + w_sent:
        copy.wait_send()
    for d in range(1, sp_n):
        ctx_copy(d).wait_send()
    for q in range(2):
        pl.when(sp + 1 < sp_n)(lambda: kv_own(sp + 1, 0, q).wait_send())
        pl.when(sp > 0)(lambda: kv_own(sp - 1, 1, q).wait_send())
    for ok, copy in sent:
        pl.when(ok)(copy.wait_send)
    for d in range(1, tp_n):
        at_copy(d).wait_send()
    phase(None)


def fused(
    axes, latent, condition, context, context_vector, modulator, norm_gain, query_weight,
    key_weight, value_weight, head_gain, lambdas, context_bias, out_weight,
):
    sp_n, tp_n, dp_n = axes
    n = sp_n * tp_n
    rows, width = latent.shape[1:]
    half = rows // 2
    chunk = modulator.shape[1] // n
    ctx_rows = context.shape[1]
    qw = query_weight.shape[1]
    value = value_weight.shape[1]
    qrows = rows * tp_n
    wrows = out_weight.shape[0] // 4
    bf, f32 = jnp.bfloat16, jnp.float32
    vm = pl.BlockSpec(memory_space=pltpu.VMEM)
    hb = pl.BlockSpec(memory_space=pltpu.HBM)
    dma = lambda k: pltpu.SemaphoreType.DMA((k,))
    result = pl.pallas_call(
        functools.partial(fused_kernel, sp_n, tp_n, (qw // 2) ** (-0.5)),
        out_shape=pltpu.VMEM((rows, width), bf),
        in_specs=[hb] * 13,
        out_specs=vm,
        scratch_shapes=[
            pltpu.VMEM(condition.shape, bf),
            pltpu.VMEM((1, context_vector.shape[0]), bf),
            pltpu.VMEM((1, width), f32),
            pltpu.VMEM((1, value), f32),
            pltpu.VMEM((1, 1), f32),
            pltpu.VMEM(context_bias.shape, f32),
            pltpu.VMEM(modulator.shape, bf),
            pltpu.VMEM((n, 2, chunk), f32),
            pltpu.VMEM((n, 2, chunk), f32),
            pltpu.VMEM((n, 2, chunk), f32),
            pltpu.VMEM((tp_n * 2, half, width), bf),
            pltpu.VMEM((sp_n, ctx_rows, width), bf),
            pltpu.VMEM((width, qw), bf),
            pltpu.VMEM((width, qw + value), bf),
            pltpu.VMEM((tp_n * 4, wrows, width), bf),
            pltpu.VMEM((8, width), f32),
            pltpu.VMEM((qrows + sp_n * ctx_rows, width), bf),
            pltpu.VMEM((sp_n * 2, qrows // 2, qw + value), bf),
            pltpu.VMEM((tp_n, rows, value), bf),
            pltpu.VMEM((tp_n, rows, value), bf),
            dma(7), dma(6), dma(1), dma(1), dma(1), dma(1), dma(6), dma(6), dma(sp_n), dma(sp_n),
            dma(4), dma(sp_n * 2), dma(sp_n * 2), dma(6), dma(6), dma(6), dma(6), dma(tp_n), dma(tp_n),
        ],
        compiler_params=pltpu.CompilerParams(
            collective_id=0, has_side_effects=True, vmem_limit_bytes=66700000
        ),
        name="fused_block",
    )(
        latent.reshape(2, half, width),
        condition,
        context[0],
        context_vector[None, :],
        modulator,
        norm_gain[None, :],
        query_weight,
        key_weight,
        value_weight,
        head_gain[None, :],
        lambdas[None, :],
        context_bias,
        out_weight.reshape(4, wrows, width),
    )
    return result[None]


def choose(axes, *arrays):
    sp_n, tp_n, dp_n = axes
    latent, modulator, query_weight, value_weight = arrays[0], arrays[4], arrays[6], arrays[8]
    lambdas, out_weight = arrays[10], arrays[12]
    fits = (
        tp_n == 4
        and dp_n == 2
        and 1 < sp_n <= 8
        and lambdas.shape[0] == 1
        and query_weight.shape[1] == LANES
        and value_weight.shape[1] == LANES
        and modulator.shape[1] % (sp_n * tp_n * LANES) == 0
        and latent.shape[1] % 32 == 0
        and latent.shape[2] % 512 == 0
        and out_weight.shape[0] % 64 == 0
    )
    return fused(axes, *arrays) if fits else body(*arrays)


def solution(mesh):
    placed = (
        P("dp", ("sp", "tp"), None),
        P("dp", ("sp", "tp")),
        P("dp", "sp", None),
        P(("sp", "tp")),
        P(("sp", "tp"), None),
        P(),
        P(None, "tp"),
        P(None, "tp"),
        P(None, "tp"),
        P(),
        P("tp"),
        P("tp", None),
        P("tp", None),
    )
    axes = (mesh.shape["sp"], mesh.shape["tp"], mesh.shape["dp"])
    return jax.shard_map(
        functools.partial(choose, axes), mesh=mesh, in_specs=placed, out_specs=P("dp", ("sp", "tp"), None), check_vma=False
    )
```

```python
import functools

import jax
import jax.numpy as jnp
from jax import lax
from jax.experimental import pallas as pl
from jax.experimental.pallas import tpu as pltpu
from jax.sharding import PartitionSpec as P

EPSILON = 1e-06
OUT_SCALE = 0.8
KEY_BLOCK = 2048
LOW_START = -1e30


def modulate(inputs, gain_vector, shift_vector, scale_vector):
    as_float = inputs.astype(jnp.float32)
    normed = as_float * lax.rsqrt(jnp.mean(as_float * as_float, axis=-1, keepdims=True) + EPSILON)
    return (normed * gain_vector * (1.0 + scale_vector) + shift_vector).astype(jnp.bfloat16)


def fold_block(running, queries, keys_in, values_in, key_flags, bias_table, score_scale):
    run_max, run_total, summed = running
    scores = (
        jnp.einsum("qhmd,khmd->hmqk", queries, keys_in, preferred_element_type=jnp.float32)
        * score_scale
    )
    if key_flags is not None:
        scores = scores + bias_table[:, :, None, None] * key_flags
    new_max = jnp.maximum(run_max, jnp.max(scores, axis=-1))
    shrink = jnp.exp(run_max - new_max)
    weights = jnp.exp(scores - new_max[..., None])
    run_total = run_total * shrink + jnp.sum(weights, axis=-1)
    summed = summed * shrink[..., None] + jnp.einsum(
        "hmqk,khe->hmqe",
        weights.astype(jnp.bfloat16),
        values_in,
        preferred_element_type=jnp.float32,
    )
    return (new_max, run_total, summed)


def fold_keys(running, queries, keys_in, values_in, key_flags, bias_table, score_scale):
    full_blocks = keys_in.shape[0] // KEY_BLOCK
    if full_blocks > 1:
        edge = full_blocks * KEY_BLOCK
        stacked = (
            keys_in[:edge].reshape((full_blocks, KEY_BLOCK) + keys_in.shape[1:]),
            values_in[:edge].reshape((full_blocks, KEY_BLOCK) + values_in.shape[1:]),
        )
        if key_flags is not None:
            stacked = stacked + (key_flags[:edge].reshape(full_blocks, KEY_BLOCK),)

        def fold_step(current, block_data):
            flag_part = None if key_flags is None else block_data[2]
            return (
                fold_block(
                    current,
                    queries,
                    block_data[0],
                    block_data[1],
                    flag_part,
                    bias_table,
                    score_scale,
                ),
                None,
            )

        running, ignored = lax.scan(fold_step, running, stacked)
        keys_in = keys_in[edge:]
        values_in = values_in[edge:]
        key_flags = None if key_flags is None else key_flags[edge:]
    if keys_in.shape[0] > 0:
        running = fold_block(
            running, queries, keys_in, values_in, key_flags, bias_table, score_scale
        )
    return running


def body(
    latent,
    condition,
    context,
    context_vector,
    modulator,
    norm_gain,
    query_weight,
    key_weight,
    value_weight,
    head_gain,
    lambdas,
    context_bias,
    out_weight,
):
    model_width = latent.shape[2]
    local_heads = lambdas.shape[0]
    query_width = query_weight.shape[1]
    head_size = query_width // (2 * local_heads)
    value_size = value_weight.shape[1] // local_heads
    score_scale = head_size ** (-0.5)
    activated = jax.nn.silu(
        jnp.concatenate([condition, context_vector[None, :]], axis=0).astype(jnp.float32)
    )
    partial_terms = jnp.dot(
        activated.astype(jnp.bfloat16), modulator, preferred_element_type=jnp.float32
    )
    modulations = lax.psum(partial_terms, ("sp", "tp"))
    hidden = modulate(
        latent[0],
        norm_gain,
        modulations[0, :model_width],
        modulations[0, model_width : 2 * model_width],
    )
    ctx_hidden = modulate(
        context[0],
        norm_gain,
        modulations[1, :model_width],
        modulations[1, model_width : 2 * model_width],
    )
    gate_vector = modulations[0, 2 * model_width :]
    incoming = lax.all_gather(hidden, "tp", axis=0, tiled=True)
    projected = jnp.concatenate(
        [
            jnp.dot(incoming, query_weight, preferred_element_type=jnp.float32),
            jnp.dot(incoming, key_weight, preferred_element_type=jnp.float32),
            jnp.dot(incoming, value_weight, preferred_element_type=jnp.float32),
        ],
        axis=1,
    ).astype(jnp.bfloat16)
    query_rows = projected.shape[0]
    queries = projected[:, :query_width].reshape(query_rows, local_heads, 2, head_size)
    own_keys = projected[:, query_width : 2 * query_width]
    own_values = projected[:, 2 * query_width :]
    gathered_context = lax.all_gather(ctx_hidden, "sp", axis=0, tiled=True)
    ctx_keys = jnp.dot(gathered_context, key_weight, preferred_element_type=jnp.float32).astype(
        jnp.bfloat16
    )
    ctx_values = jnp.dot(gathered_context, value_weight, preferred_element_type=jnp.float32).astype(
        jnp.bfloat16
    )
    start_carry = (
        jnp.full((local_heads, 2, query_rows), LOW_START, jnp.float32),
        jnp.zeros((local_heads, 2, query_rows), jnp.float32),
        jnp.zeros((local_heads, 2, query_rows, value_size), jnp.float32),
    )
    pieces = (own_keys, own_values)
    initial = fold_keys(
        start_carry,
        queries,
        ctx_keys.reshape(-1, local_heads, 2, head_size),
        ctx_values.reshape(-1, local_heads, value_size),
        jnp.ones((ctx_keys.shape[0],), jnp.float32),
        context_bias,
        score_scale,
    )
    incoming = (
        lax.all_gather(pieces[0], "sp", axis=0, tiled=True),
        lax.all_gather(pieces[1], "sp", axis=0, tiled=True),
    )
    run_max, run_total, summed = fold_keys(
        initial,
        queries,
        incoming[0].reshape(-1, local_heads, 2, head_size),
        incoming[1].reshape(-1, local_heads, value_size),
        None,
        context_bias,
        score_scale,
    )
    mixed = (
        summed[:, 0] / run_total[:, 0, :, None]
        - lambdas[:, None, None] * summed[:, 1] / run_total[:, 1, :, None]
    )
    normed = (
        mixed
        * lax.rsqrt(jnp.mean(mixed * mixed, axis=-1, keepdims=True) + EPSILON)
        * head_gain
        * OUT_SCALE
    )
    attended = (
        jnp.transpose(normed, (1, 0, 2))
        .reshape(query_rows, local_heads * value_size)
        .astype(jnp.bfloat16)
    )
    exchanged = lax.all_to_all(attended, "tp", split_axis=0, concat_axis=1, tiled=True)
    whole_weight = lax.all_gather(out_weight, "tp", axis=0, tiled=True)
    branch = jnp.dot(exchanged, whole_weight, preferred_element_type=jnp.float32)
    result = (latent[0].astype(jnp.float32) + gate_vector * branch).astype(jnp.bfloat16)
    return result[None]


MESH = pl.DeviceIdType.MESH
LANES = 128


class Phases:
    def __init__(self):
        self.open = None

    def __call__(self, name):
        if self.open is not None:
            self.open.__exit__(None, None, None)
        self.open = None
        if name is not None:
            self.open = jax.named_scope(name)
            self.open.__enter__()


def fused_kernel(
    sp_n, tp_n, score_scale,
    latent, condition_in, context, vector_in, modulator, gain_in,
    query_weight, key_weight, value_weight, head_gain_in, lambdas_in, bias_in, out_weight,
    out,
    condition, context_vector, norm_gain, head_gain, lambdas, context_bias,
    mod_v, part, rs_in, mods, lat, ctx_all, w_q, w_kv, w_out, vecs, hid, kvb, att_out, att_in,
    small_sem, own_sem, rs_ss, rs_rs, ag_ss, ag_rs, lat_ss, lat_rs, ctx_ss, ctx_rs,
    kv_os, kv_ss, kv_rs, wt_ss, wt_rs, wd_ss, wd_rs, at_ss, at_rs,
):
    sp = lax.axis_index("sp")
    tp = lax.axis_index("tp")
    dp = lax.axis_index("dp")
    n = sp_n * tp_n
    rank = sp * tp_n + tp
    across = tp + 1 - 2 * lax.rem(tp, 2)
    along = lax.rem(tp + 2, 4)
    corner = along + 1 - 2 * lax.rem(along, 2)
    roles = (tp, across, along, corner)
    half = lat.shape[1]
    width = lat.shape[2]
    rows = half * 2
    qrows = rows * tp_n
    chunk = part.shape[2]

    phase = Phases()
    phase("enter")
    barrier = pltpu.get_barrier_semaphore()

    small = [
        pltpu.make_async_copy(source, place, small_sem.at[k])
        for k, (source, place) in enumerate((
            (condition_in, condition), (vector_in, context_vector), (context, ctx_all.at[sp]),
            (gain_in, norm_gain), (head_gain_in, head_gain), (lambdas_in, lambdas),
            (bias_in, context_bias),
        ))
    ]
    loads = [
        pltpu.make_async_copy(modulator, mod_v, own_sem.at[0]),
        pltpu.make_async_copy(latent, lat.at[pl.ds(tp * 2, 2)], own_sem.at[1]),
        pltpu.make_async_copy(key_weight, w_kv.at[:, pl.ds(0, LANES)], own_sem.at[2]),
        pltpu.make_async_copy(value_weight, w_kv.at[:, pl.ds(LANES, LANES)], own_sem.at[3]),
        pltpu.make_async_copy(query_weight, w_q, own_sem.at[4]),
        pltpu.make_async_copy(out_weight, w_out.at[pl.ds(tp * 4, 4)], own_sem.at[5]),
    ]
    for load in small[:2] + loads[:2] + small[2:] + loads[2:]:
        load.start()

    def greet(d, carry):
        peer = lax.rem(rank + d, n)
        pl.semaphore_signal(
            barrier, inc=1, device_id=(peer // tp_n, lax.rem(peer, tp_n), dp), device_id_type=MESH
        )
        return carry

    lax.fori_loop(1, n, greet, 0)
    pl.semaphore_signal(barrier, inc=1, device_id=(sp, tp, 1 - dp), device_id_type=MESH)

    phase("partial")
    for load in small:
        load.wait()
    rows_in = jnp.concatenate([condition[...], context_vector[...]], axis=0).astype(jnp.float32)
    activated = jax.nn.silu(rows_in).astype(jnp.bfloat16)
    loads[0].wait()
    partial_terms = jnp.dot(activated, mod_v[...], preferred_element_type=jnp.float32)
    for p in range(n):
        part[p] = partial_terms[:, p * chunk : (p + 1) * chunk]
    loads[1].wait()
    phase("barrier")
    pl.semaphore_wait(barrier, n)
    phase("sends")

    def rs_copy(d):
        peer = lax.rem(rank + d, n)
        return pltpu.make_async_remote_copy(
            src_ref=part.at[peer], dst_ref=rs_in.at[d], send_sem=rs_ss.at[0], recv_sem=rs_rs.at[0],
            device_id=(peer // tp_n, lax.rem(peer, tp_n), dp), device_id_type=MESH,
        )

    def ag_copy(d):
        peer = lax.rem(rank + d, n)
        return pltpu.make_async_remote_copy(
            src_ref=mods.at[rank], dst_ref=mods.at[rank], send_sem=ag_ss.at[0], recv_sem=ag_rs.at[0],
            device_id=(peer // tp_n, lax.rem(peer, tp_n), dp), device_id_type=MESH,
        )

    def rs_all():
        return pltpu.make_async_remote_copy(
            src_ref=part.at[pl.ds(0, n - 1)], dst_ref=rs_in.at[pl.ds(1, n - 1)],
            send_sem=rs_ss.at[0], recv_sem=rs_rs.at[0],
            device_id=(sp, across, dp), device_id_type=MESH,
        )

    def ag_all():
        return pltpu.make_async_remote_copy(
            src_ref=mods.at[pl.ds(0, n - 1)], dst_ref=mods.at[pl.ds(0, n - 1)],
            send_sem=ag_ss.at[0], recv_sem=ag_rs.at[0],
            device_id=(sp, across, dp), device_id_type=MESH,
        )

    def each(first, last, act):
        def step(d, carry):
            act(d)
            return carry

        lax.fori_loop(first, last, step, 0)

    each(1, n, lambda d: rs_copy(d).start())


    class Plane:
        def __init__(self, buf, index, ss, rs):
            self.buf, self.index, self.ss, self.rs = buf, index, ss, rs

        def copy(self, owner, part_no, target, slot, kind):
            place = self.buf.at[self.index(owner, part_no)]
            return pltpu.make_async_remote_copy(
                src_ref=place, dst_ref=place, send_sem=self.ss.at[slot],
                recv_sem=self.rs.at[kind * 2 + part_no],
                device_id=(sp, target, dp), device_id_type=MESH,
            )

        def first(self):
            return [
                self.copy(tp, 0, across, 0, 0),
                self.copy(tp, 1, along, 1, 1),
                self.copy(tp, 1, across, 2, 0),
                self.copy(tp, 0, along, 3, 1),
            ]

        def relays(self):
            return [self.copy(across, 0, along, 4, 2), self.copy(along, 1, across, 5, 2)]

        def arrival(self, kind, part_no):
            owner = (across, along, corner)[kind]
            return self.copy(owner, part_no, across, 0, kind)

    plane = Plane(lat, lambda o, q: o * 2 + q, lat_ss, lat_rs)
    lat_first = plane.first()
    for copy in lat_first:
        copy.start()

    def ctx_copy(d):
        peer = lax.rem(sp + d, sp_n)
        return pltpu.make_async_remote_copy(
            src_ref=ctx_all.at[sp], dst_ref=ctx_all.at[sp], send_sem=ctx_ss.at[d], recv_sem=ctx_rs.at[d],
            device_id=(peer, tp, dp), device_id_type=MESH,
        )

    def ctx_arrival(d):
        peer = lax.rem(sp - d + sp_n, sp_n)
        return pltpu.make_async_remote_copy(
            src_ref=ctx_all.at[peer], dst_ref=ctx_all.at[peer], send_sem=ctx_ss.at[d], recv_sem=ctx_rs.at[d],
            device_id=(peer, tp, dp), device_id_type=MESH,
        )

    for d in range(1, sp_n):
        ctx_copy(d).start()
    rs_in[0] = part[rank]

    phase("rs_wait")
    rs_all().wait_recv()
    total = rs_in[0]
    for d in range(1, n):
        total = total + rs_in[d]
    mods[rank] = total
    each(1, n, lambda d: ag_copy(d).start())

    phase("lat_relay")
    lat_relays = plane.relays()
    plane.arrival(0, 0).wait_recv()
    lat_relays[0].start()
    plane.arrival(1, 1).wait_recv()
    lat_relays[1].start()

    loads[5].wait()
    wplane = Plane(w_out, lambda o, q: o * 4 + dp * 2 + q, wt_ss, wt_rs)
    w_first = wplane.first()
    for copy in w_first:
        copy.start()

    for d in range(1, sp_n):
        ctx_arrival(d).wait_recv()
    phase("ag_wait")
    ag_all().wait_recv()
    whole = jnp.concatenate([mods[p] for p in range(n)], axis=1)
    phase("vecs")
    gain = norm_gain[...]
    vecs[0:1, :] = gain * (1.0 + whole[0:1, width : 2 * width])
    vecs[1:2, :] = whole[0:1, :width]
    vecs[2:3, :] = gain * (1.0 + whole[1:2, width : 2 * width])
    vecs[3:4, :] = whole[1:2, :width]
    vecs[4:5, :] = whole[0:1, 2 * width :]

    def normed_rows(x, at):
        x = x.astype(jnp.float32)
        scale = lax.rsqrt(jnp.mean(x * x, axis=-1, keepdims=True) + EPSILON)
        return (x * scale * vecs[at : at + 1, :] + vecs[at + 1 : at + 2, :]).astype(jnp.bfloat16)

    def norm_block(role):
        for q in range(2):
            at = (role * 2 + q) * half
            hid[at : at + half, :] = normed_rows(lat[roles[role] * 2 + q], 0)

    def kv_own(to, slot, q):
        place = kvb.at[sp * 2 + q]
        return pltpu.make_async_remote_copy(
            src_ref=place, dst_ref=place, send_sem=kv_os.at[slot * 2 + q],
            recv_sem=kv_rs.at[sp * 2 + q], device_id=(to, tp, dp), device_id_type=MESH,
        )

    def kv_rows(first, last):
        product = jnp.dot(hid[first:last, :], w_kv[...], preferred_element_type=jnp.float32)
        return product.astype(jnp.bfloat16)

    def kv_send(q):
        pl.when(sp + 1 < sp_n)(lambda: kv_own(sp + 1, 0, q).start())
        pl.when(sp > 0)(lambda: kv_own(sp - 1, 1, q).start())

    piece = qrows // 2
    ctx_rows = ctx_all.shape[0] * ctx_all.shape[1]
    norm_block(0)
    plane.arrival(0, 1).wait_recv()
    norm_block(1)
    phase("kv0")
    for load in loads[2:5]:
        load.wait()
    kv_near = kv_rows(0, piece)
    kvb[sp * 2] = kv_near
    kv_send(0)
    phase("lat_rest")
    hid[qrows : qrows + ctx_rows, :] = normed_rows(
        ctx_all[...].astype(jnp.float32).reshape(ctx_rows, width), 2
    )
    plane.arrival(1, 0).wait_recv()
    norm_block(2)
    plane.arrival(2, 0).wait_recv()
    plane.arrival(2, 1).wait_recv()
    norm_block(3)
    phase("kv1")
    kv_far = kv_rows(piece, qrows + ctx_rows)
    kvb[sp * 2 + 1] = kv_far[:piece]
    kv_send(1)
    kv = jnp.concatenate([kv_near, kv_far[:piece]], axis=0)
    ctx_kv = kv_far[piece:]

    phase("queries")
    queries = jnp.dot(hid[:qrows, :], w_q[...], preferred_element_type=jnp.float32) * score_scale
    queries = queries.astype(jnp.bfloat16)
    head = queries.shape[1] // 2
    lane = lax.broadcasted_iota(jnp.int32, queries.shape, 1)
    zero = jnp.zeros_like(queries)
    both = jnp.concatenate(
        [jnp.where(lane < head, queries, zero), jnp.where(lane < head, zero, queries)], axis=0
    )

    def score(keys):
        return lax.dot_general(
            both, keys, (((1,), (1,)), ((), ())), preferred_element_type=jnp.float32
        )

    map_row = lax.broadcasted_iota(jnp.int32, (2 * qrows, 1), 0)
    bias = jnp.where(map_row < qrows, context_bias[0:1, 0:1], context_bias[0:1, 1:2])

    def fold(running, scores, values):
        top = jnp.max(scores, axis=-1, keepdims=True)
        if running is not None:
            top = jnp.maximum(running[0], top)
        weights = jnp.exp(scores - top)
        count = jnp.sum(weights, axis=-1, keepdims=True)
        summed = jnp.dot(weights.astype(jnp.bfloat16), values, preferred_element_type=jnp.float32)
        if running is not None:
            shrink = jnp.exp(running[0] - top)
            count = running[1] * shrink + count
            summed = running[2] * shrink + summed
        return top, count, summed

    phase("fold_own")
    running = fold(None, score(ctx_kv[:, :LANES]) + bias, ctx_kv[:, LANES:])
    running = fold(running, score(kv[:, :LANES]), kv[:, LANES:])

    def sibling(owner, part_no, slot):
        place = w_out.at[owner * 4 + dp * 2 + part_no]
        return pltpu.make_async_remote_copy(
            src_ref=place, dst_ref=place, send_sem=wd_ss.at[slot], recv_sem=wd_rs.at[slot],
            device_id=(sp, tp, 1 - dp), device_id_type=MESH,
        )

    def sibling_arrival(owner, part_no, slot):
        place = w_out.at[owner * 4 + (1 - dp) * 2 + part_no]
        return pltpu.make_async_remote_copy(
            src_ref=place, dst_ref=place, send_sem=wd_ss.at[slot], recv_sem=wd_rs.at[slot],
            device_id=(sp, tp, 1 - dp), device_id_type=MESH,
        )

    owners = (across, along, corner)
    w_sent = []

    def swap(kind, part_no, wait=True):
        if wait:
            wplane.arrival(kind, part_no).wait_recv()
        copy = sibling(owners[kind], part_no, kind * 2 + part_no)
        copy.start()
        w_sent.append(copy)

    high = (2 * sp) // sp_n

    def block_at(t):
        up = (t - 1) + jnp.where(t - 1 >= sp, 1, 0)
        down = (sp_n - t) - jnp.where(sp_n - t <= sp, 1, 0)
        return jnp.where(high == 0, up, down)

    def onward(b, q):
        step = jnp.where(b < sp, 1, -1)
        to = sp + step
        ok = jnp.logical_and(to >= 0, to < sp_n)
        safe = jnp.where(ok, to, sp - step)
        return ok, pltpu.make_async_remote_copy(
            src_ref=kvb.at[b * 2 + q], dst_ref=kvb.at[b * 2 + q], send_sem=kv_ss.at[b * 2 + q],
            recv_sem=kv_rs.at[b * 2 + q], device_id=(safe, tp, dp), device_id_type=MESH,
        )

    sent = []
    def take(t, q):
        ok, copy = onward(block_at(t), q)
        copy.wait_recv()
        pl.when(ok)(copy.start)
        sent.append((ok, copy))

    near = [t for t in (1, 2) if t < sp_n]
    phase("take_near")
    for t in near:
        take(t, 0)
    phase("w_relay")
    w_relays = wplane.relays()
    wplane.arrival(0, 0).wait_recv()
    w_relays[0].start()
    wplane.arrival(1, 1).wait_recv()
    w_relays[1].start()
    swap(0, 0, False)
    swap(1, 1, False)

    phase("take_near2")
    for t in near:
        take(t, 1)
    swap(0, 1)
    swap(1, 0)
    phase("fold_near")
    for t in near:
        block = kvb[pl.ds(block_at(t) * 2, 2)].reshape(qrows, 2 * LANES)
        running = fold(running, score(block[:, :LANES]), block[:, LANES:])
    for t in range(3, sp_n):
        for q in range(2):
            phase(f"take{t}_{q}")
            take(t, q)
            block = kvb[block_at(t) * 2 + q]
            running = fold(running, score(block[:, :LANES]), block[:, LANES:])

    phase("finish")
    top, count, summed = running
    shares = summed / count
    mixed = shares[:qrows] - lambdas[...] * shares[qrows:]
    normed = (
        mixed
        * lax.rsqrt(jnp.mean(mixed * mixed, axis=-1, keepdims=True) + EPSILON)
        * head_gain[...]
        * OUT_SCALE
    ).astype(jnp.bfloat16)
    for p in range(tp_n):
        att_out[p] = normed[p * rows : (p + 1) * rows]

    def at_copy(d):
        return pltpu.make_async_remote_copy(
            src_ref=att_out.at[d], dst_ref=att_in.at[tp], send_sem=at_ss.at[d], recv_sem=at_rs.at[d],
            device_id=(sp, roles[d], dp), device_id_type=MESH,
        )

    def at_arrival(d):
        return pltpu.make_async_remote_copy(
            src_ref=att_out.at[d], dst_ref=att_in.at[roles[d]], send_sem=at_ss.at[d],
            recv_sem=at_rs.at[d], device_id=(sp, roles[d], dp), device_id_type=MESH,
        )

    for d in (3, 1, 2):
        at_copy(d).start()
    att_in[tp] = att_out[0]

    phase("w_wait")
    swap(2, 0)
    swap(2, 1)
    for kind in range(3):
        for part_no in range(2):
            sibling_arrival(owners[kind], part_no, kind * 2 + part_no).wait_recv()
    phase("at_wait")
    for d in range(1, tp_n):
        at_arrival(d).wait_recv()

    phase("out")
    attended = jnp.concatenate([att_in[p] for p in range(tp_n)], axis=1)
    step = 512
    for first in range(0, width, step):
        cols = slice(first, first + step)
        weight = w_out[:, :, cols].reshape(attended.shape[1], step)
        branch = jnp.dot(attended, weight, preferred_element_type=jnp.float32)
        for q in range(2):
            mine = lat[tp * 2 + q, :, cols].astype(jnp.float32)
            update = mine + vecs[4:5, cols] * branch[q * half : (q + 1) * half]
            out[q * half : (q + 1) * half, cols] = update.astype(jnp.bfloat16)

    phase("drain")
    rs_all().wait_send()
    ag_all().wait_send()
    for copy in lat_first + lat_relays + w_first + w_relays + w_sent:
        copy.wait_send()
    for d in range(1, sp_n):
        ctx_copy(d).wait_send()
    for q in range(2):
        pl.when(sp + 1 < sp_n)(lambda: kv_own(sp + 1, 0, q).wait_send())
        pl.when(sp > 0)(lambda: kv_own(sp - 1, 1, q).wait_send())
    for ok, copy in sent:
        pl.when(ok)(copy.wait_send)
    for d in range(1, tp_n):
        at_copy(d).wait_send()
    phase(None)


def fused(
    axes, latent, condition, context, context_vector, modulator, norm_gain, query_weight,
    key_weight, value_weight, head_gain, lambdas, context_bias, out_weight,
):
    sp_n, tp_n, dp_n = axes
    n = sp_n * tp_n
    rows, width = latent.shape[1:]
    half = rows // 2
    chunk = modulator.shape[1] // n
    ctx_rows = context.shape[1]
    qw = query_weight.shape[1]
    value = value_weight.shape[1]
    qrows = rows * tp_n
    wrows = out_weight.shape[0] // 4
    bf, f32 = jnp.bfloat16, jnp.float32
    vm = pl.BlockSpec(memory_space=pltpu.VMEM)
    hb = pl.BlockSpec(memory_space=pltpu.HBM)
    dma = lambda k: pltpu.SemaphoreType.DMA((k,))
    result = pl.pallas_call(
        functools.partial(fused_kernel, sp_n, tp_n, (qw // 2) ** (-0.5)),
        out_shape=pltpu.VMEM((rows, width), bf),
        in_specs=[hb] * 13,
        out_specs=vm,
        scratch_shapes=[
            pltpu.VMEM(condition.shape, bf),
            pltpu.VMEM((1, context_vector.shape[0]), bf),
            pltpu.VMEM((1, width), f32),
            pltpu.VMEM((1, value), f32),
            pltpu.VMEM((1, 1), f32),
            pltpu.VMEM(context_bias.shape, f32),
            pltpu.VMEM(modulator.shape, bf),
            pltpu.VMEM((n, 2, chunk), f32),
            pltpu.VMEM((n, 2, chunk), f32),
            pltpu.VMEM((n, 2, chunk), f32),
            pltpu.VMEM((tp_n * 2, half, width), bf),
            pltpu.VMEM((sp_n, ctx_rows, width), bf),
            pltpu.VMEM((width, qw), bf),
            pltpu.VMEM((width, qw + value), bf),
            pltpu.VMEM((tp_n * 4, wrows, width), bf),
            pltpu.VMEM((8, width), f32),
            pltpu.VMEM((qrows + sp_n * ctx_rows, width), bf),
            pltpu.VMEM((sp_n * 2, qrows // 2, qw + value), bf),
            pltpu.VMEM((tp_n, rows, value), bf),
            pltpu.VMEM((tp_n, rows, value), bf),
            dma(7), dma(6), dma(1), dma(1), dma(1), dma(1), dma(6), dma(6), dma(sp_n), dma(sp_n),
            dma(4), dma(sp_n * 2), dma(sp_n * 2), dma(6), dma(6), dma(6), dma(6), dma(tp_n), dma(tp_n),
        ],
        compiler_params=pltpu.CompilerParams(
            collective_id=0, has_side_effects=True, vmem_limit_bytes=66700000
        ),
        name="fused_block",
    )(
        latent.reshape(2, half, width),
        condition,
        context[0],
        context_vector[None, :],
        modulator,
        norm_gain[None, :],
        query_weight,
        key_weight,
        value_weight,
        head_gain[None, :],
        lambdas[None, :],
        context_bias,
        out_weight.reshape(4, wrows, width),
    )
    return result[None]


def choose(axes, *arrays):
    sp_n, tp_n, dp_n = axes
    latent, modulator, query_weight, value_weight = arrays[0], arrays[4], arrays[6], arrays[8]
    lambdas, out_weight = arrays[10], arrays[12]
    fits = (
        tp_n == 4
        and dp_n == 2
        and 1 < sp_n <= 8
        and lambdas.shape[0] == 1
        and query_weight.shape[1] == LANES
        and value_weight.shape[1] == LANES
        and modulator.shape[1] % (sp_n * tp_n * LANES) == 0
        and latent.shape[1] % 32 == 0
        and latent.shape[2] % 512 == 0
        and out_weight.shape[0] % 64 == 0
    )
    return fused(axes, *arrays) if fits else body(*arrays)


def solution(mesh):
    placed = (
        P("dp", ("sp", "tp"), None),
        P("dp", ("sp", "tp")),
        P("dp", "sp", None),
        P(("sp", "tp")),
        P(("sp", "tp"), None),
        P(),
        P(None, "tp"),
        P(None, "tp"),
        P(None, "tp"),
        P(),
        P("tp"),
        P("tp", None),
        P("tp", None),
    )
    axes = (mesh.shape["sp"], mesh.shape["tp"], mesh.shape["dp"])
    return jax.shard_map(
        functools.partial(choose, axes), mesh=mesh, in_specs=placed, out_specs=P("dp", ("sp", "tp"), None), check_vma=False
    )
```
